32 devices in a mesh: ep: 8 (over z, x), tp: 4 (over y, core).
Axes of the slice: x: 2, y: 2, z: 4, core: 2. Of those that a mesh axis runs over, the one named last changes fastest.
Arguments:
- queries: bfloat16 [1024, 4096], P('ep', 'tp'), may hold values from -112 to 112
- key_rows: bfloat16 [1024, 4096], P('ep', 'tp'), may hold values from -8.1 to 8.1
- values: bfloat16 [1024, 4096], P('ep', 'tp'), may hold values from -6 to 6
- lambdas: float32 [16], P('tp'), may hold values from 0.3 to 0.8
- head_gain: float32 [256], replicated, may hold values from 0.1 to 1.9
- tokens: bfloat16 [512, 4096], P('ep'), may hold values from -6 to 6
- moe_gain: float32 [4096], replicated, may hold values from 0.1 to 1.9
- routes: int32 [512, 2], P('ep'), may hold values from 0 to 7, all different within a row; in each aligned block of 64 rows (0 to 63, 64 to 127, ...) at most 32 rows name the same one
- route_scores: float32 [512, 2], P('ep'), may hold values from -6 to 6
- w_gate: bfloat16 [8, 4096, 2048], P('ep', None, 'tp'), may hold values from -0.09375 to 0.09375
- w_up: bfloat16 [8, 4096, 2048], P('ep', None, 'tp'), may hold values from -0.09375 to 0.09375
- w_down: bfloat16 [8, 2048, 4096], P('ep', 'tp'), may hold values from -0.125 to 0.125
Outputs:
- attended: bfloat16 [1024, 4096], P('ep', 'tp')
- expert_out: bfloat16 [512, 4096], P('ep', 'tp')
The draws below stay inside these ranges and needn't reach their ends.
Inputs may be any that keep to these rules, and one draw needn't show every extreme that they name: `routes`: each row names 2 different experts. Among the rows of one index of ep at most 32 name the same expert, and some index reaches 32 in every draw.
All inputs are finite; a program needn't handle non-finite values.
Results may differ from the reference program's by a relative error of at most 0.018.
Values may be sent and summed in bfloat16 or wider, within the bound.
No kernel may reach another device: no remote copies, remote signals or barrier semaphores. Data moves between devices by JAX's collectives and lax.ppermute only.
A program may use at most 64 MiB of HBM per device.

```python
import math
from functools import partial
import jax
import jax.numpy as jnp
import numpy as np
from jax import lax

D = 4096
HEADS = 16
QKD = 128
VD = 256
FF = 2048
TOP = 2
TOKB_DEV = 64
SEQ = 1024
TOKB = 512
EXPERTS = 8
CAP = 32
N_EP = 8
N_TP = 4


def base_pairs(key):
    seed_one, seed_two, seed_three, seed_four, seed_five = jax.random.split(jax.random.fold_in(key, 11), 5)
    row_width = HEADS * 2 * QKD
    queries = jnp.clip(jax.random.normal(seed_one, (SEQ, row_width), jnp.float32) * 1.3, -8.0, 8.0)
    key_rows = jnp.clip(jax.random.normal(seed_two, (SEQ, row_width), jnp.float32) * 1.3, -8.0, 8.0)
    return (queries, key_rows, seed_three, seed_four, seed_five)


def draw_queries(key, part):
    drawn = base_pairs(key)
    return drawn[0].astype(jnp.bfloat16)


def draw_key_rows(key, part):
    drawn = base_pairs(key)
    return drawn[1].astype(jnp.bfloat16)


def block_levels(own_key, shape, cuts, smallest, largest):
    gain = 1.0
    for dim, parts in cuts:
        heights = jax.random.uniform(jax.random.fold_in(jax.random.fold_in(own_key, 6), dim), (parts,), jnp.float32, smallest / len(cuts), largest / len(cuts))
        gain = gain * jnp.repeat(jnp.exp(heights), shape[dim] // parts).reshape((-1,) + (1,) * (len(shape) - 1 - dim))
    return gain


def shared_out(rng, own, number, rows, amount, top, reach, lean):
    ranking = jax.random.permutation(rng, amount)
    heavy_load, usual = shares(amount, rows * top, reach, lean, True), shares(amount, rows * top, reach, lean, False)
    places = jnp.arange(amount)

    def named(tallies, offset_by):
        used = int((tallies > 0).sum())
        fixed = max(1, used // 4)
        passed = fixed + (places - fixed + offset_by * (used - fixed)) % max(1, amount - fixed)
        return jnp.zeros((amount,), jnp.int32).at[ranking[jnp.where(places < fixed, places, passed)]].set(jnp.asarray(tallies, jnp.int32))

    tallies = jnp.where(number % 4 == 0, named(heavy_load, number // 4), named(usual, number - number // 4 - 1))
    mixed = jax.random.permutation(jax.random.fold_in(own, 3), amount)
    giver, sink = mixed[0:amount // 2 * 2:2], mixed[1:amount // 2 * 2:2]
    margin = jnp.minimum(tallies[giver] - 1, reach - tallies[sink]) // 2
    margin = jnp.where((giver == ranking[0]) | (sink == ranking[0]) | (tallies[sink] == 0), 0, jnp.maximum(margin, 0))
    passed = jax.random.randint(jax.random.fold_in(own, 4), (amount // 2,), 0, 1 << 20) % (margin + 1)
    tallies = tallies.at[giver].add(-passed).at[sink].add(passed)
    members = jnp.searchsorted(jnp.cumsum(tallies), jnp.arange(rows * top), side="right").astype(jnp.int32)
    grid = members.reshape(top, rows).T
    grid = grid[jax.random.permutation(jax.random.fold_in(own, 1), rows)]
    offset_by = jax.random.randint(jax.random.fold_in(own, 2), (rows, 1), 0, top)
    return jnp.take_along_axis(grid, (jnp.arange(top)[None, :] + offset_by) % top, axis=1)


def shares(number_of, total, reach, slope, full):
    loads = [(1 << 20) // math.isqrt(standing ** slope) + 1 for standing in range(1, number_of + 1)]
    largest = reach if full else min(reach, max(-(-total // number_of), total * loads[0] // sum(loads)))
    least = 1 if total - largest >= number_of - 1 else 0
    given, spare = [largest] + [least] * (number_of - 1), total - largest - least * (number_of - 1)
    while spare > 0:
        candidates = [i for i in range(1, number_of) if given[i] < largest] or [i for i in range(1, number_of) if given[i] < reach]
        whole, budget = sum([loads[i] for i in candidates]), spare
        for i in candidates:
            extra = min(reach - given[i], max(1, budget * loads[i] // whole), spare)
            given[i] = given[i] + extra
            spare = spare - extra
    return np.array(given)


def bell_draw(own_key, dims, spread, limit, pieces=(), held_as=jnp.bfloat16):
    array = spread * jax.random.normal(own_key, dims, jnp.float32)
    if pieces:
        array = array * block_levels(own_key, dims, pieces, -0.22, 0.18)
    return jnp.clip(array, -limit, limit).astype(held_as)


def setup_inputs(seed: int = 0) -> dict:
    arg_keys = jax.random.split(jax.random.key(seed), 13)
    queries = draw_queries(jax.random.fold_in(arg_keys[12], 71), 0)
    key_rows = draw_key_rows(jax.random.fold_in(arg_keys[12], 71), 0)
    values = bell_draw(arg_keys[2], (SEQ, HEADS * VD), 1.0, 6.0, ((0, 8), (1, 4)))
    lambdas = jnp.clip(0.3 + 0.5 * jax.random.uniform(arg_keys[3], (HEADS,), jnp.float32) ** block_levels(arg_keys[3], (HEADS,), ((0, 4),), -0.2, 0.2), 0.3, 0.8)
    head_gain = jnp.clip(1.0 + 0.18 * jax.random.normal(arg_keys[4], (VD,), jnp.float32), 0.1, 1.9)
    tokens = bell_draw(arg_keys[5], (TOKB, D), 1.0, 6.0, ((0, 8),))
    moe_gain = jnp.clip(1.0 + 0.18 * jax.random.normal(arg_keys[6], (D,), jnp.float32), 0.1, 1.9)
    routes_keys = jax.random.split(jax.random.fold_in(arg_keys[7], 1), TOKB // TOKB_DEV)
    routes_turns = jax.random.permutation(jax.random.fold_in(arg_keys[7], 3), TOKB // TOKB_DEV)
    routes = jax.vmap(lambda own, number: shared_out(jax.random.fold_in(arg_keys[7], 2), own, number, TOKB_DEV, EXPERTS, TOP, CAP, 1))(routes_keys, routes_turns).reshape((TOKB, TOP))
    route_scores = bell_draw(arg_keys[8], (TOKB, TOP), 1.0, 6.0, ((0, 8),), jnp.float32)
    w_gate = bell_draw(arg_keys[9], (EXPERTS, D, FF), D ** -0.5, 0.09375, ((0, 8), (2, 4)))
    w_up = bell_draw(arg_keys[10], (EXPERTS, D, FF), D ** -0.5, 0.09375, ((0, 8), (2, 4)))
    w_down = bell_draw(arg_keys[11], (EXPERTS, FF, D), FF ** -0.5, 0.125, ((0, 8), (1, 4)))
    return {"queries": queries, "key_rows": key_rows, "values": values, "lambdas": lambdas, "head_gain": head_gain, "tokens": tokens, "moe_gain": moe_gain, "routes": routes, "route_scores": route_scores, "w_gate": w_gate, "w_up": w_up, "w_down": w_down}


neg_big = -1e+30
head_eps = 1e-05
moe_eps = 1e-06
head_scale = 0.8

def slot_table(routes, experts, capacity):
    flat_routes = routes.reshape(-1)
    onehot = (flat_routes[:, None] == jnp.arange(experts, dtype=jnp.int32)[None, :]).astype(jnp.int32)
    before = jnp.cumsum(onehot, axis=0) - onehot
    position = lax.optimization_barrier(jnp.sum(before * onehot, axis=1))
    return (flat_routes * capacity + position).astype(jnp.int32).reshape(routes.shape)

def reference(queries, key_rows, values, lambdas, head_gain, tokens, moe_gain, routes, route_scores, w_gate, w_up, w_down):
    query_heads = queries.reshape(SEQ, HEADS, 2, QKD).transpose(1, 0, 2, 3)
    key_heads = key_rows.reshape(SEQ, HEADS, 2, QKD).transpose(1, 0, 2, 3)
    value_heads = values.reshape(SEQ, HEADS, VD).transpose(1, 0, 2)
    visible = jnp.tril(jnp.ones((SEQ, SEQ), dtype=bool))

    def one_head(inputs):
        query_h, key_h, value_h, weight_h = inputs
        scores = jnp.einsum('qmd,kmd->mqk', query_h.astype(jnp.float32), key_h.astype(jnp.float32), precision=lax.Precision.HIGHEST) * QKD ** (-0.5)
        scores = jnp.where(visible[None], scores, neg_big)
        probabilities = jax.nn.softmax(scores, axis=-1)
        mixing = probabilities[0] - weight_h * probabilities[1]
        mixed_out = jnp.dot(mixing, value_h.astype(jnp.float32), precision=lax.Precision.HIGHEST)
        scaled = mixed_out * lax.rsqrt(lax.optimization_barrier(jnp.mean(mixed_out * mixed_out, axis=-1, keepdims=True)) + head_eps)
        return (scaled * head_gain * head_scale).astype(jnp.bfloat16)
    heads_out = lax.map(one_head, (query_heads, key_heads, value_heads, lambdas))
    attended = heads_out.transpose(1, 0, 2).reshape(SEQ, HEADS * VD)
    token_f32 = tokens.astype(jnp.float32)
    normed = (token_f32 * lax.rsqrt(lax.optimization_barrier(jnp.mean(token_f32 * token_f32, axis=-1, keepdims=True)) + moe_eps) * moe_gain).astype(jnp.bfloat16)
    gate_weights = jax.nn.softmax(route_scores, axis=-1)
    local_slots = jax.vmap(partial(slot_table, experts=EXPERTS, capacity=CAP))(routes.reshape(N_EP, TOKB_DEV, TOP))
    expert_ids = local_slots // CAP
    within = local_slots % CAP
    source = jnp.arange(N_EP, dtype=jnp.int32)[:, None, None]
    global_slot = (expert_ids * (N_EP * CAP) + source * CAP + within).astype(jnp.int32).reshape(TOKB, TOP)
    row_ids = jnp.broadcast_to(jnp.arange(TOKB, dtype=jnp.int32)[:, None], (TOKB, TOP))
    row_of_slot = jnp.zeros((EXPERTS * N_EP * CAP,), jnp.int32).at[global_slot.reshape(-1)].set(row_ids.reshape(-1))
    gathered = normed[row_of_slot].reshape(EXPERTS, N_EP * CAP, D)
    group_size = FF // N_TP

    def one_expert(inputs):
        rows_e, gate_e, up_e, down_e = inputs
        gate_act = jnp.dot(rows_e, gate_e, preferred_element_type=jnp.float32)
        up_act = jnp.dot(rows_e, up_e, preferred_element_type=jnp.float32)
        hidden = (jax.nn.silu(gate_act) * up_act).astype(jnp.bfloat16)

        def add_group(group_index, running):
            offset = (group_index * group_size).astype(jnp.int32)
            hidden_part = lax.dynamic_slice_in_dim(hidden, offset, group_size, 1)
            down_part = lax.dynamic_slice_in_dim(down_e, offset, group_size, 0)
            partial_sum = jnp.dot(hidden_part, down_part, preferred_element_type=jnp.float32).astype(jnp.bfloat16)
            partial_sum = lax.optimization_barrier(partial_sum)
            return running + partial_sum.astype(jnp.float32)
        running = lax.fori_loop(jnp.int32(0), jnp.int32(N_TP), add_group, jnp.zeros((N_EP * CAP, D), jnp.float32))
        return running.astype(jnp.bfloat16)
    results = lax.map(one_expert, (gathered, w_gate, w_up, w_down)).reshape(EXPERTS * N_EP * CAP, D)
    picked = results[global_slot].astype(jnp.float32)
    expert_out = lax.optimization_barrier(jnp.sum(gate_weights[..., None] * picked, axis=1)).astype(jnp.bfloat16)
    return (attended, expert_out)
```

```python
import functools

import jax
import jax.numpy as jnp
from jax import lax
from jax.experimental import pallas as pl
from jax.experimental.pallas import tpu as pltpu
from jax.sharding import PartitionSpec as P

QKD = 128
VD = 256
TOP = 2


neg_big = -1e30
head_eps = 1e-05
moe_eps = 1e-06
head_scale = 0.8

VMEM = pl.BlockSpec(memory_space=pltpu.VMEM)
SMEM = pl.BlockSpec(memory_space=pltpu.SMEM)


def struct(shape, dtype=jnp.bfloat16):
    return jax.ShapeDtypeStruct(shape, dtype)


def params():
    return pltpu.CompilerParams(vmem_limit_bytes=48 * 1024 * 1024)


def dot(a, b, contract=((1,), (0,))):
    return lax.dot_general(a, b, (contract, ((), ())), preferred_element_type=jnp.float32)


def block_expert(lane, place, nx):
    z, x = place
    return ((lane // nx) ^ z) * nx + ((lane % nx) ^ x)


def prep_kernel(nz, nx, cap, width, place_ref, tokens_ref, gain_ref, routes_ref, *out_refs):
    z, x, tp = place_ref[0], place_ref[1], place_ref[2]
    blocks = nz * nx
    rows = tokens_ref.shape[0]
    tokens = tokens_ref[...].astype(jnp.float32)
    scale = lax.rsqrt(jnp.mean(tokens * tokens, axis=-1, keepdims=True) + moe_eps)
    columns = pl.ds(pl.multiple_of(tp * width, width), width)
    normed = (tokens_ref[:, columns].astype(jnp.float32) * scale * gain_ref[:, columns]).astype(
        jnp.bfloat16
    )
    lane = lax.broadcasted_iota(jnp.int32, (rows, 128), 1)
    wanted = jnp.where(lane < blocks, block_expert(lane, (z, x), nx), -1)
    hit = (routes_ref[:, 0:1] == wanted) | (routes_ref[:, 1:2] == wanted)
    hit = jnp.where(hit, 1.0, 0.0).astype(jnp.bfloat16)
    row_from = lax.broadcasted_iota(jnp.int32, (rows, rows), 0)
    row_to = lax.broadcasted_iota(jnp.int32, (rows, rows), 1)
    same = jnp.where(row_from == row_to, 1.0, 0.0).astype(jnp.bfloat16)
    before = jnp.where(row_from < row_to, 1.0, 0.0).astype(jnp.bfloat16)
    hit_t = dot(hit, same, ((0,), (0,)))[:blocks]
    place_t = dot(hit, before, ((0,), (0,)))[:blocks].astype(jnp.int32)
    slot = lax.broadcasted_iota(jnp.int32, (blocks, cap, rows), 1)
    picker = (hit_t[:, None, :] > 0.5) & (place_t[:, None, :] == slot)
    picker = jnp.where(picker, 1.0, 0.0).reshape(blocks * cap, rows).astype(jnp.bfloat16)
    picked = dot(picker, normed).astype(jnp.bfloat16)
    for j in range(blocks):
        out_refs[j][...] = picked[j * cap : (j + 1) * cap]


def gates_kernel(nz, nx, cap, place_ref, routes_ref, scores_ref, high_ref, low_ref):
    z, x = place_ref[0], place_ref[1]
    rows = routes_ref.shape[0]
    slots = nz * nx * cap
    scores = scores_ref[...]
    scores = jnp.exp(scores - jnp.max(scores, axis=-1, keepdims=True))
    gates = scores / jnp.sum(scores, axis=-1, keepdims=True)
    lane = lax.broadcasted_iota(jnp.int32, (rows, slots), 1)
    wanted = block_expert(lane // cap, (z, x), nx)
    first = routes_ref[:, 0:1] == wanted
    second = routes_ref[:, 1:2] == wanted
    row_from = lax.broadcasted_iota(jnp.int32, (rows, rows), 1)
    row_to = lax.broadcasted_iota(jnp.int32, (rows, rows), 0)
    before = jnp.where(row_from < row_to, 1.0, 0.0).astype(jnp.bfloat16)
    hit = jnp.where(first | second, 1.0, 0.0).astype(jnp.bfloat16)
    place = dot(before, hit).astype(jnp.int32)
    weight = jnp.where(first, gates[:, 0:1], jnp.where(second, gates[:, 1:2], 0.0))
    weight = jnp.where(place == lane % cap, weight, 0.0)
    high = weight.astype(jnp.bfloat16)
    high_ref[...] = high
    low_ref[...] = (weight - high.astype(jnp.float32)).astype(jnp.bfloat16)


def combine_kernel(cap, high_ref, low_ref, *refs):
    out_ref, held = refs[-2], refs[-1]
    for j, ref in enumerate(refs[:-2]):
        held[j * cap : (j + 1) * cap, :] = ref[...]
    returned = held[...]
    out_ref[...] = (dot(high_ref[...], returned) + dot(low_ref[...], returned)).astype(jnp.bfloat16)


def expert_kernel(tp_n, groups, group_rows, sub, place_ref, *refs):
    n_in = tp_n * groups
    row_refs = refs[:n_in]
    gate_ref, up_ref, down_ref = refs[n_in : n_in + 3]
    out_refs = refs[n_in + 3 : n_in + 3 + tp_n]
    gate_acc, up_acc, hidden = refs[n_in + 3 + tp_n :]
    step = pl.program_id(0)
    depth = gate_ref.shape[0]

    @pl.when(step == 0)
    def _():
        gate_acc[...] = jnp.zeros_like(gate_acc)
        up_acc[...] = jnp.zeros_like(up_acc)

    for i in range(tp_n * sub):
        q, s = divmod(i, sub)

        @pl.when(step == i)
        def _():
            rows = [row_refs[q * groups + g][:, s * depth : (s + 1) * depth] for g in range(groups)]
            rows = jnp.concatenate(rows, axis=0)
            gate_acc[...] += dot(rows, gate_ref[...])
            up_acc[...] += dot(rows, up_ref[...])

    @pl.when(step == tp_n * sub)
    def _():
        gate = gate_acc[...]
        hidden[...] = (gate * jax.nn.sigmoid(gate) * up_acc[...]).astype(jnp.bfloat16)

    for q in range(tp_n):

        @pl.when(step == tp_n * sub + q)
        def _():
            out_refs[q][...] = dot(hidden[...], down_ref[...]).astype(jnp.bfloat16)


def run_experts(place, parts, w_gate, w_up, w_down, tp_n):
    groups = len(parts[0])
    group_rows, width = parts[0][0].shape
    total = groups * group_rows
    model, units = w_gate.shape
    sub = 2 if width % 256 == 0 and width > 256 else 1
    depth = width // sub
    last = tp_n * sub - 1

    def up_index(i, place_ref):
        j = jnp.minimum(i, last)
        return ((j // sub) ^ place_ref[2]) * sub + j % sub, 0

    def down_index(i, place_ref):
        return 0, jnp.maximum(i - tp_n * sub, 0) ^ place_ref[2]

    whole = lambda shape: pl.BlockSpec(shape, lambda i, place_ref: (0,) * len(shape))
    flat = [part for column in parts for part in column]
    return pl.pallas_call(
        functools.partial(expert_kernel, tp_n, groups, group_rows, sub),
        out_shape=[struct((total, width))] * tp_n,
        grid_spec=pltpu.PrefetchScalarGridSpec(
            num_scalar_prefetch=1,
            grid=(tp_n * sub + tp_n,),
            in_specs=[whole((group_rows, width))] * len(flat)
            + [
                pl.BlockSpec((depth, units), up_index),
                pl.BlockSpec((depth, units), up_index),
                pl.BlockSpec((units, width), down_index),
            ],
            out_specs=[whole((total, width))] * tp_n,
            scratch_shapes=[
                pltpu.VMEM((total, units), jnp.float32),
                pltpu.VMEM((total, units), jnp.float32),
                pltpu.VMEM((total, units), jnp.bfloat16),
            ],
        ),
        compiler_params=params(),
        name="experts",
    )(place, *flat, w_gate, w_up, w_down)


def pack_kernel(nz, wide, place_ref, queries_ref, keys_ref, values_ref, *out_refs):
    z = place_ref[0]
    rows = queries_ref.shape[0]
    for k in range(nz):
        columns = pl.ds(pl.multiple_of((z ^ k) * wide, wide), wide)
        out_refs[k][...] = queries_ref[:, columns]
        out_refs[nz + k][:rows, :] = keys_ref[:, columns]
        out_refs[nz + k][rows:, :] = values_ref[:, columns]


def attend_kernel(nz, nx, heads, place_ref, lambda_ref, gain_ref, *refs):
    query_refs = refs[:nz]
    pair_refs = refs[nz : nz + nz * nx]
    out_refs = refs[nz + nz * nx : 2 * nz + nz * nx]
    query_s, key_s, value_s, out_s = refs[2 * nz + nz * nx :]
    z, x = place_ref[0], place_ref[1]
    rows = query_refs[0].shape[0]

    def at(block):
        return pl.ds(pl.multiple_of(block * rows, rows), rows)

    for k in range(nz):
        query_s[at(z ^ k), :] = query_refs[k][...]
        for m in range(nx):
            block = at((z ^ k) * nx + (x ^ m))
            key_s[block, :] = pair_refs[k * nx + m][:rows, :]
            value_s[block, :] = pair_refs[k * nx + m][rows:, :]
    for head in range(heads):
        weight = lambda_ref[z * heads + head]
        for group in range(nz):
            count = (group + 1) * nx * rows
            query_pos = (group * nx + x) * rows + lax.broadcasted_iota(jnp.int32, (rows, count), 0)
            visible = lax.broadcasted_iota(jnp.int32, (rows, count), 1) <= query_pos
            maps = []
            for index in range(2):
                lanes = slice(head * VD + index * QKD, head * VD + (index + 1) * QKD)
                scores = dot(
                    query_s[group * rows : (group + 1) * rows, lanes],
                    key_s[:count, lanes],
                    ((1,), (1,)),
                )
                scores = jnp.where(visible, scores * QKD ** (-0.5), neg_big)
                weights = jnp.exp(scores - jnp.max(scores, axis=-1, keepdims=True))
                maps.append((weights, jnp.sum(weights, axis=-1, keepdims=True)))
            mixing = maps[0][0] * (1.0 / maps[0][1]) - maps[1][0] * (weight / maps[1][1])
            lanes = slice(head * VD, (head + 1) * VD)
            high = mixing.astype(jnp.bfloat16)
            low = (mixing - high.astype(jnp.float32)).astype(jnp.bfloat16)
            held = value_s[:count, lanes]
            mixed = dot(high, held) + dot(low, held)
            scaled = mixed * lax.rsqrt(jnp.mean(mixed * mixed, axis=-1, keepdims=True) + head_eps)
            scaled = scaled * gain_ref[...] * head_scale
            out_s[group * rows : (group + 1) * rows, lanes] = scaled.astype(jnp.bfloat16)
    for k in range(nz):
        out_refs[k][...] = out_s[at(z ^ k), :]


def join_kernel(nz, wide, place_ref, *refs):
    z = place_ref[0]
    for k in range(nz):
        refs[-1][:, pl.ds(pl.multiple_of((z ^ k) * wide, wide), wide)] = refs[k][...]


def fold_block(query_group, query_pos, key_heads, value_heads, key_pos):
    scores = jnp.einsum(
        "qhmd,khmd->hmqk", query_group, key_heads, preferred_element_type=jnp.float32
    ) * QKD ** (-0.5)
    visible = key_pos[None, :] <= query_pos[:, None]
    scores = jnp.where(visible, scores, neg_big)
    weights = jnp.where(visible, jnp.exp(scores - jnp.max(scores, axis=-1, keepdims=True)), 0.0)
    accumulated = jnp.einsum(
        "hmqk,khd->hmqd", weights, value_heads, precision=lax.Precision.HIGHEST
    )
    return jnp.sum(weights, axis=-1), accumulated


def gathered_attention(queries, key_rows, values, lambdas, head_gain):
    rows = queries.shape[0]
    heads = lambdas.shape[0]
    half = rows // 2
    keys = lax.all_gather(key_rows, "ep", axis=0, tiled=True)
    held = lax.all_gather(values, "ep", axis=0, tiled=True)
    count = keys.shape[0]
    keys = keys.reshape(count, heads, 2, QKD)
    held = held.reshape(count, heads, VD).astype(jnp.float32)
    key_pos = jnp.arange(count, dtype=jnp.int32)
    groups = []
    for g in range(2):
        pos = lax.axis_index("ep") * rows + g * half + jnp.arange(half, dtype=jnp.int32)
        group = queries[g * half : (g + 1) * half].reshape(half, heads, 2, QKD)
        total, mixed = fold_block(group, pos, keys, held, key_pos)
        mixed = mixed / total[..., None]
        mixed = mixed[:, 0] - lambdas[:, None, None] * mixed[:, 1]
        scaled = mixed * lax.rsqrt(jnp.mean(mixed * mixed, axis=-1, keepdims=True) + head_eps)
        scaled = scaled * head_gain * head_scale
        groups.append(scaled.transpose(1, 0, 2).reshape(half, heads * VD).astype(jnp.bfloat16))
    return jnp.concatenate(groups, axis=0)


def local(
    sizes,
    queries,
    key_rows,
    values,
    lambdas,
    head_gain,
    tokens,
    moe_gain,
    routes,
    route_scores,
    w_gate,
    w_up,
    w_down,
):
    nz, nx, tp_n = sizes
    ep_n = nz * nx
    ep, tp = lax.axis_index("ep"), lax.axis_index("tp")
    place = jnp.stack([ep // nx, ep % nx, tp]).astype(jnp.int32)
    rows_b, model = tokens.shape
    cap = 2 * TOP * rows_b // ep_n
    width = model // tp_n

    def over_z(v, k):
        return v if k == 0 else lax.ppermute(v, "ep", [(i, i ^ (k * nx)) for i in range(ep_n)])

    def over_x(v, m):
        return v if m == 0 else lax.ppermute(v, "ep", [(i, i ^ m) for i in range(ep_n)])

    def over_tp(v, q):
        return v if q == 0 else lax.ppermute(v, "tp", [(i, i ^ q) for i in range(tp_n)])

    sends = pl.pallas_call(
        functools.partial(prep_kernel, nz, nx, cap, width),
        out_shape=[struct((cap, width))] * ep_n,
        in_specs=[SMEM, VMEM, VMEM, VMEM],
        out_specs=[VMEM] * ep_n,
        compiler_params=params(),
        name="prep",
    )(place, tokens, moe_gain.reshape(1, model), routes)

    order = list(range(nx - 1, -1, -1))
    groups = {}
    for m in order:
        groups[m] = [over_z(sends[k * nx + m], k) for k in range(nz)]

    split_heads = lambdas.shape[0] % nz == 0
    if split_heads:
        heads = lambdas.shape[0] // nz
        wide = heads * VD
        rows_a = queries.shape[0]
        packs = pl.pallas_call(
            functools.partial(pack_kernel, nz, wide),
            out_shape=[struct((rows_a, wide))] * nz + [struct((2 * rows_a, wide))] * nz,
            in_specs=[SMEM, VMEM, VMEM, VMEM],
            out_specs=[VMEM] * (2 * nz),
            compiler_params=params(),
            name="pack",
        )(place, queries, key_rows, values)
        pairs = [over_z(packs[nz + k], k) for k in range(nz)]
        asked = [over_z(packs[k], k) for k in range(nz)]

    groups = {m: over_x(jnp.concatenate(groups[m], axis=0), m) for m in order}
    parts = {}
    for q in range(0, tp_n, 2):
        for m in order:
            parts[q, m] = over_tp(groups[m], q)
    for q in range(0, tp_n, 2):
        for m in order:
            parts[q + 1, m] = over_tp(parts[q, m], 1)

    if split_heads:
        swapped = [[over_x(pair, m) for m in range(nx)] for pair in pairs]
        outs = pl.pallas_call(
            functools.partial(attend_kernel, nz, nx, heads),
            out_shape=[struct((rows_a, wide))] * nz,
            in_specs=[SMEM, SMEM] + [VMEM] * (1 + nz + nz * nx),
            out_specs=[VMEM] * nz,
            scratch_shapes=[
                pltpu.VMEM((nz * rows_a, wide), jnp.bfloat16),
                pltpu.VMEM((ep_n * rows_a, wide), jnp.bfloat16),
                pltpu.VMEM((ep_n * rows_a, wide), jnp.bfloat16),
                pltpu.VMEM((nz * rows_a, wide), jnp.bfloat16),
            ],
            compiler_params=params(),
            name="attend",
        )(place, lambdas, head_gain.reshape(1, VD), *asked, *[v for pair in swapped for v in pair])
        outs = [over_z(outs[k], k) for k in range(nz)]
        attended = pl.pallas_call(
            functools.partial(join_kernel, nz, wide),
            out_shape=struct((rows_a, nz * wide)),
            in_specs=[SMEM] + [VMEM] * nz,
            out_specs=VMEM,
            compiler_params=params(),
            name="join",
        )(place, *outs)
    else:
        attended = gathered_attention(queries, key_rows, values, lambdas, head_gain)

    results = run_experts(
        place,
        [[parts[q, m] for m in order] for q in range(tp_n)],
        w_gate[0],
        w_up[0],
        w_down[0],
        tp_n,
    )
    sums = {}
    for q in list(range(2, tp_n, 2)) + [0]:
        other = over_tp(results[q + 1], 1)
        sums[q] = results[q].astype(jnp.float32) + other.astype(jnp.float32)
    span = nz * cap
    returned = {}
    for g, m in enumerate(order):
        total = sums[0][g * span : (g + 1) * span]
        for q in range(2, tp_n, 2):
            piece = sums[q][g * span : (g + 1) * span].astype(jnp.bfloat16)
            total = total + over_tp(piece, q).astype(jnp.float32)
        total = over_x(total.astype(jnp.bfloat16), m)
        for k in range(nz):
            returned[k, m] = over_z(total[k * cap : (k + 1) * cap], k)

    high, low = pl.pallas_call(
        functools.partial(gates_kernel, nz, nx, cap),
        out_shape=[struct((rows_b, ep_n * cap))] * 2,
        in_specs=[SMEM, VMEM, VMEM],
        out_specs=[VMEM, VMEM],
        compiler_params=params(),
        name="gates",
    )(place, routes, route_scores)
    expert_out = pl.pallas_call(
        functools.partial(combine_kernel, cap),
        out_shape=struct((rows_b, width)),
        in_specs=[VMEM] * (2 + ep_n),
        out_specs=VMEM,
        scratch_shapes=[pltpu.VMEM((ep_n * cap, width), jnp.bfloat16)],
        compiler_params=params(),
        name="combine",
    )(high, low, *[returned[k, m] for k in range(nz) for m in range(nx)])
    return attended, expert_out


def solution(mesh):
    ep_n, tp_n = mesh.shape["ep"], mesh.shape["tp"]
    nx = 1
    while (2 * nx) * (2 * nx) <= ep_n:
        nx *= 2
    return jax.shard_map(
        functools.partial(local, (ep_n // nx, nx, tp_n)),
        mesh=mesh,
        in_specs=(
            P("ep", "tp"),
            P("ep", "tp"),
            P("ep", "tp"),
            P("tp"),
            P(),
            P("ep", None),
            P(),
            P("ep", None),
            P("ep", None),
            P("ep", None, "tp"),
            P("ep", None, "tp"),
            P("ep", "tp", None),
        ),
        out_specs=(P("ep", "tp"), P("ep", "tp")),
        check_vma=False,
    )
```

```python
import functools

import jax
import jax.numpy as jnp
from jax import lax
from jax.experimental import pallas as pl
from jax.experimental.pallas import tpu as pltpu
from jax.sharding import PartitionSpec as P


QKD = 128
VD = 256
TOP = 2


neg_big = -1e30
head_eps = 1e-05
moe_eps = 1e-06
head_scale = 0.8

VMEM = pl.BlockSpec(memory_space=pltpu.VMEM)
SMEM = pl.BlockSpec(memory_space=pltpu.SMEM)
HBM = pl.BlockSpec(memory_space=pltpu.HBM)


def struct(shape, dtype=jnp.bfloat16):
    return jax.ShapeDtypeStruct(shape, dtype)


def params(mib=8):
    return pltpu.CompilerParams(vmem_limit_bytes=mib * 1024 * 1024)


def dot(a, b, contract=((1,), (0,))):
    return lax.dot_general(a, b, (contract, ((), ())), preferred_element_type=jnp.float32)


def where_am_i(nx):
    ep = lax.axis_index("ep")
    return lax.div(ep, nx), lax.rem(ep, nx), lax.axis_index("tp")


def slot_hits(nz, nx, cap, routes):
    z, x, _ = where_am_i(nx)
    blocks, rows = nz * nx, routes.shape[1]
    block = lax.broadcasted_iota(jnp.int32, (blocks, rows), 0)
    wanted = (lax.div(block, nx) ^ z) * nx + (lax.rem(block, nx) ^ x)
    first, second = routes[0:1, :] == wanted, routes[1:2, :] == wanted
    hit = jnp.where(first | second, 1.0, 0.0)
    row_from = lax.broadcasted_iota(jnp.int32, (rows, rows), 0)
    row_to = lax.broadcasted_iota(jnp.int32, (rows, rows), 1)
    before = jnp.where(row_from < row_to, 1.0, 0.0).astype(jnp.bfloat16)
    place = jnp.where(hit > 0.5, dot(hit.astype(jnp.bfloat16), before), -1.0)
    slot = lax.broadcasted_iota(jnp.int32, (blocks, cap, rows), 1).astype(jnp.float32)
    return place[:, None, :] == slot, first


def prep_kernel(nz, nx, cap, width, wide, tokens_ref, gain_ref, routes_ref, *refs):
    blocks = nz * nx
    tokens_s, gain_s, sems = refs[-3:]
    copies = [
        pltpu.make_async_copy(tokens_ref, tokens_s, sems.at[0]),
        pltpu.make_async_copy(gain_ref, gain_s, sems.at[1]),
    ]
    slices = []
    if wide:
        z = where_am_i(nx)[0]
        sources, refs = refs[:3], refs[3:]
        count = sources[0].shape[0]
        for k in range(nz):
            columns = pl.ds(pl.multiple_of((z ^ k) * wide, wide), wide)
            for i, source in enumerate(sources):
                target = refs[blocks + k].at[pl.ds(i * count, count), :]
                sem = sems.at[2 + 3 * k + i]
                slices.append(pltpu.make_async_copy(source.at[:, columns], target, sem))
    out_refs = refs[:blocks]
    for copy in copies + slices:
        copy.start()
    rows = tokens_ref.shape[0]
    picker, _ = slot_hits(nz, nx, cap, routes_ref[...])
    picker = jnp.where(picker, 1.0, 0.0).reshape(blocks * cap, rows).astype(jnp.bfloat16)
    for copy in copies:
        copy.wait()
    tokens = tokens_s[...].astype(jnp.float32)
    scale = lax.rsqrt(jnp.mean(tokens * tokens, axis=-1, keepdims=True) + moe_eps)
    columns = pl.ds(pl.multiple_of(lax.axis_index("tp") * width, width), width)
    normed = tokens_s[:, columns].astype(jnp.float32) * scale * gain_s[:, columns]
    picked = dot(picker, normed.astype(jnp.bfloat16)).astype(jnp.bfloat16)
    for j in range(blocks):
        out_refs[j][...] = picked[j * cap : (j + 1) * cap]
    for copy in slices:
        copy.wait()


def gates_kernel(nz, nx, cap, routes_ref, scores_ref, high_ref, low_ref):
    rows = routes_ref.shape[1]
    scores = scores_ref[...]
    scores = jnp.exp(scores - jnp.max(scores, axis=0, keepdims=True))
    gates = scores / jnp.sum(scores, axis=0, keepdims=True)
    taken, first = slot_hits(nz, nx, cap, routes_ref[...])
    weight = jnp.where(first, gates[0:1, :], gates[1:2, :])
    weight = jnp.where(taken, weight[:, None, :], 0.0).reshape(nz * nx * cap, rows)
    high = weight.astype(jnp.bfloat16)
    high_ref[...] = high
    low_ref[...] = (weight - high.astype(jnp.float32)).astype(jnp.bfloat16)


def blend_kernel(nz, cap, n_sums, *refs):
    sum_refs, refs = refs[:n_sums], refs[n_sums:]
    attend_refs, near_ref, out_refs = refs[: nz - 1], refs[nz - 1], refs[nz:]
    total = sum_refs[0][...].astype(jnp.float32)
    for ref in sum_refs[1:]:
        total = total + ref[...].astype(jnp.float32)
    total = total.astype(jnp.bfloat16)
    near_ref[...] = total[:cap]
    for k in range(1, nz):
        out_ref = out_refs[k - 1]
        count, wide = attend_refs[k - 1].shape
        out_ref[:count, :] = attend_refs[k - 1][...]
        for c in range(total.shape[1] // wide):
            out_ref[count + c * cap : count + (c + 1) * cap, :] = total[
                k * cap : (k + 1) * cap, c * wide : (c + 1) * wide
            ]


def finish_kernel(nz, nx, cap, wide, high_ref, low_ref, *refs):
    blocks, refs = refs[: nz * nx], refs[nz * nx :]
    *refs, held, out_s, sems = refs
    copies = []
    if wide:
        own_ref, out_ref, attended_ref = refs
        z = where_am_i(nx)[0]
        count = own_ref.shape[0]
        for k in range(nz):
            source = blocks[k * nx].at[pl.ds(0, count), :] if k else own_ref
            columns = pl.ds(pl.multiple_of((z ^ k) * wide, wide), wide)
            copies.append(pltpu.make_async_copy(source, attended_ref.at[:, columns], sems.at[k]))
    else:
        (out_ref,) = refs
    for copy in copies:
        copy.start()
    for j, ref in enumerate(blocks):
        slots = slice(j * cap, (j + 1) * cap)
        if wide and j >= nx and j % nx == 0:
            for c in range(held.shape[1] // wide):
                first = count + c * cap
                held[slots, c * wide : (c + 1) * wide] = ref[first : first + cap, :]
        else:
            held[slots, :] = ref[...]
    returned = held[...]
    rows = ((0,), (0,))
    out_s[...] = (
        dot(high_ref[...], returned, rows) + dot(low_ref[...], returned, rows)
    ).astype(jnp.bfloat16)
    copies.append(pltpu.make_async_copy(out_s, out_ref, sems.at[nz]))
    copies[-1].start()
    for copy in copies:
        copy.wait()


def fence_kernel(in_ref, out_ref):
    out_ref[...] = in_ref[...]


def early_kernel(groups, tp_n, *refs):
    row_refs = refs[: 2 * groups]
    gate_ref, up_ref, down_ref = refs[2 * groups : 2 * groups + 3]
    gate_out, up_out, gate_late, up_late, down_late = refs[2 * groups + 3 : 2 * groups + 8]
    gate_s, up_s, sems = refs[2 * groups + 8 :]
    width = row_refs[0].shape[1]
    tp = lax.axis_index("tp")

    def block(q):
        return pl.ds(pl.multiple_of((tp ^ q) * width, width), width)

    early, late = [], []
    for q in range(tp_n):
        for which, (source, held, later) in enumerate(
            ((gate_ref, gate_s, gate_late), (up_ref, up_s, up_late))
        ):
            target = held.at[q] if q < 2 else later.at[q - 2]
            copy = pltpu.make_async_copy(source.at[block(q), :], target, sems.at[which, q])
            (early if q < 2 else late).append(copy)
    for q in range(tp_n):
        late.append(
            pltpu.make_async_copy(down_ref.at[:, block(q)], down_late.at[q], sems.at[2, q])
        )
    for copy in early + late:
        copy.start()
    gate, up = 0.0, 0.0
    for q in range(2):
        rows = [row_refs[q * groups + g][...] for g in range(groups)]
        rows = jnp.concatenate(rows, axis=0)
        early[2 * q].wait()
        gate = gate + dot(rows, gate_s[q])
        early[2 * q + 1].wait()
        up = up + dot(rows, up_s[q])
    gate_out[...] = gate
    up_out[...] = up
    for copy in late:
        copy.wait()


def late_kernel(groups, tp_n, *refs):
    n_in = (tp_n - 2) * groups
    row_refs = refs[:n_in]
    gate_in, up_in, gate_ref, up_ref, down_ref = refs[n_in : n_in + 5]
    out_refs = refs[n_in + 5 :]
    gate, up = gate_in[...], up_in[...]
    for q in range(tp_n - 2):
        rows = [row_refs[q * groups + g][...] for g in range(groups)]
        rows = jnp.concatenate(rows, axis=0)
        gate = gate + dot(rows, gate_ref[q])
        up = up + dot(rows, up_ref[q])
    hidden = (gate * jax.nn.sigmoid(gate) * up).astype(jnp.bfloat16)
    size = hidden.shape[0] // groups
    for q in range(tp_n):
        result = dot(hidden, down_ref[q]).astype(jnp.bfloat16)
        for g in range(groups):
            out_refs[q * groups + g][...] = result[g * size : (g + 1) * size]


def attend_kernel(nz, nx, heads, place_ref, lambda_ref, gain_ref, *refs):
    pack_refs = refs[:nz]
    near_refs = refs[nz : nz + nx - 1]
    rest_refs = refs[nz + nx - 1 : nz + 2 * (nx - 1)]
    out_refs = refs[nz + 2 * (nx - 1) : 2 * nz + 2 * (nx - 1)]
    query_s, key_s, value_s, out_s = refs[2 * nz + 2 * (nx - 1) :]
    z, x = place_ref[0], place_ref[1]
    rows = pack_refs[0].shape[0] // 3

    def at(block):
        return pl.ds(pl.multiple_of(block * rows, rows), rows)

    for k in range(nz):
        query_s[at(z ^ k), :] = pack_refs[k][2 * rows :, :]
        for m in range(nx):
            if m == 0:
                source, first = pack_refs[k], 0
            elif k == 0:
                source, first = near_refs[m - 1], 0
            else:
                source, first = rest_refs[m - 1], (k - 1) * 2 * rows
            block = at((z ^ k) * nx + (x ^ m))
            key_s[block, :] = source[first : first + rows, :]
            value_s[block, :] = source[first + rows : first + 2 * rows, :]
    for head in range(heads):
        weight = lambda_ref[z * heads + head]
        for group in range(nz):
            count = (group + 1) * nx * rows
            query_pos = (group * nx + x) * rows + lax.broadcasted_iota(jnp.int32, (rows, count), 0)
            visible = lax.broadcasted_iota(jnp.int32, (rows, count), 1) <= query_pos
            maps = []
            for index in range(2):
                lanes = slice(head * VD + index * QKD, head * VD + (index + 1) * QKD)
                scores = dot(
                    query_s[group * rows : (group + 1) * rows, lanes],
                    key_s[:count, lanes],
                    ((1,), (1,)),
                )
                scores = jnp.where(visible, scores * QKD ** (-0.5), neg_big)
                weights = jnp.exp(scores - jnp.max(scores, axis=-1, keepdims=True))
                maps.append((weights, jnp.sum(weights, axis=-1, keepdims=True)))
            mixing = maps[0][0] * (1.0 / maps[0][1]) - maps[1][0] * (weight / maps[1][1])
            lanes = slice(head * VD, (head + 1) * VD)
            high = mixing.astype(jnp.bfloat16)
            low = (mixing - high.astype(jnp.float32)).astype(jnp.bfloat16)
            held = value_s[:count, lanes]
            mixed = dot(high, held) + dot(low, held)
            scaled = mixed * lax.rsqrt(jnp.mean(mixed * mixed, axis=-1, keepdims=True) + head_eps)
            scaled = scaled * gain_ref[...] * head_scale
            out_s[group * rows : (group + 1) * rows, lanes] = scaled.astype(jnp.bfloat16)
    for k in range(nz):
        out_refs[k][...] = out_s[at(z ^ k), :]


def fold_block(query_group, query_pos, key_heads, value_heads, key_pos):
    scores = jnp.einsum(
        "qhmd,khmd->hmqk", query_group, key_heads, preferred_element_type=jnp.float32
    ) * QKD ** (-0.5)
    visible = key_pos[None, :] <= query_pos[:, None]
    scores = jnp.where(visible, scores, neg_big)
    weights = jnp.where(visible, jnp.exp(scores - jnp.max(scores, axis=-1, keepdims=True)), 0.0)
    accumulated = jnp.einsum(
        "hmqk,khd->hmqd", weights, value_heads, precision=lax.Precision.HIGHEST
    )
    return jnp.sum(weights, axis=-1), accumulated


def gathered_attention(queries, key_rows, values, lambdas, head_gain):
    rows = queries.shape[0]
    heads = lambdas.shape[0]
    half = rows // 2
    keys = lax.all_gather(key_rows, "ep", axis=0, tiled=True)
    held = lax.all_gather(values, "ep", axis=0, tiled=True)
    count = keys.shape[0]
    keys = keys.reshape(count, heads, 2, QKD)
    held = held.reshape(count, heads, VD).astype(jnp.float32)
    key_pos = jnp.arange(count, dtype=jnp.int32)
    groups = []
    for g in range(2):
        pos = lax.axis_index("ep") * rows + g * half + jnp.arange(half, dtype=jnp.int32)
        group = queries[g * half : (g + 1) * half].reshape(half, heads, 2, QKD)
        total, mixed = fold_block(group, pos, keys, held, key_pos)
        mixed = mixed / total[..., None]
        mixed = mixed[:, 0] - lambdas[:, None, None] * mixed[:, 1]
        scaled = mixed * lax.rsqrt(jnp.mean(mixed * mixed, axis=-1, keepdims=True) + head_eps)
        scaled = scaled * head_gain * head_scale
        groups.append(scaled.transpose(1, 0, 2).reshape(half, heads * VD).astype(jnp.bfloat16))
    return jnp.concatenate(groups, axis=0)


def local(
    sizes,
    queries,
    key_rows,
    values,
    lambdas,
    head_gain,
    tokens,
    moe_gain,
    routes,
    route_scores,
    w_gate,
    w_up,
    w_down,
):
    nz, nx, tp_n = sizes
    ep_n = nz * nx
    ep = lax.axis_index("ep")
    place = jnp.stack([ep // nx, ep % nx]).astype(jnp.int32)
    rows_b, model = tokens.shape
    cap = 2 * TOP * rows_b // ep_n
    width = model // tp_n
    units = w_gate.shape[2]

    def shift(v, axis, mask):
        if mask == 0:
            return v
        n = ep_n if axis == "ep" else tp_n
        return lax.ppermute(v, axis, [(i, i ^ mask) for i in range(n)])

    def kernel(body, ins, outs, in_specs=None, out_specs=None, scratch=(), mib=8):
        if in_specs:
            ins = [
                pltpu.with_memory_space_constraint(v, pltpu.HBM) if spec is HBM else v
                for v, spec in zip(ins, in_specs)
            ]
        return pl.pallas_call(
            body,
            out_shape=outs,
            in_specs=in_specs or [VMEM] * len(ins),
            out_specs=out_specs or jax.tree.map(lambda _: VMEM, outs),
            scratch_shapes=scratch,
            compiler_params=params(mib),
        )(*ins)

    heads, odd = divmod(lambdas.shape[0], nz)
    wide = 0 if odd or width % (heads * VD) else heads * VD
    rows_a = queries.shape[0]
    slices = (key_rows, values, queries) if wide else ()
    sends = kernel(
        functools.partial(prep_kernel, nz, nx, cap, width, wide),
        (tokens, moe_gain.reshape(1, model), routes.T, *slices),
        [struct((cap, width))] * ep_n + [struct((3 * rows_a, wide))] * (nz if wide else 0),
        in_specs=[HBM, HBM, VMEM] + [HBM] * len(slices),
        scratch=[
            pltpu.VMEM((rows_b, model), jnp.bfloat16),
            pltpu.VMEM((1, model), jnp.float32),
            pltpu.SemaphoreType.DMA((2 + 3 * nz,)),
        ],
    )
    sends, packs = sends[:ep_n], sends[ep_n:]
    order = list(range(1, nx)) + [0]
    parts = {}
    for m in order:
        arrived = [shift(sends[k * nx + m], "ep", k * nx + m) for k in range(nz)]
        parts[0, m] = jnp.concatenate(arrived, axis=0)

    packs = [shift(pack, "ep", k * nx) for k, pack in enumerate(packs)]

    for q in range(0, tp_n, 2):
        for m in order:
            parts[q, m] = shift(parts[0, m], "tp", q)
            parts[q + 1, m] = shift(parts[q, m], "tp", 1)

    attended = None
    if wide:
        near = packs[0][: 2 * rows_a]
        rest = jnp.concatenate([pack[: 2 * rows_a] for pack in packs[1:]], axis=0)
        near = [shift(near, "ep", m) for m in range(1, nx)]
        rest = [shift(rest, "ep", m) for m in range(1, nx)]
        gain = kernel(fence_kernel, (head_gain.reshape(1, VD),), struct((1, VD), jnp.float32))
        outs = kernel(
            functools.partial(attend_kernel, nz, nx, heads),
            (place, lambdas, gain, *packs, *near, *rest),
            [struct((rows_a, wide))] * nz,
            in_specs=[SMEM, SMEM] + [VMEM] * (1 + nz + 2 * (nx - 1)),
            scratch=[
                pltpu.VMEM((nz * rows_a, wide), jnp.bfloat16),
                pltpu.VMEM((ep_n * rows_a, wide), jnp.bfloat16),
                pltpu.VMEM((ep_n * rows_a, wide), jnp.bfloat16),
                pltpu.VMEM((nz * rows_a, wide), jnp.bfloat16),
            ],
            mib=16,
        )
    else:
        attended = gathered_attention(queries, key_rows, values, lambdas, head_gain)

    slots = ep_n * cap
    gate, up, *late = kernel(
        functools.partial(early_kernel, nx, tp_n),
        (*[parts[q, m] for q in range(2) for m in order], w_gate[0], w_up[0], w_down[0]),
        [
            struct((slots, units), jnp.float32),
            struct((slots, units), jnp.float32),
            struct((tp_n - 2, width, units)),
            struct((tp_n - 2, width, units)),
            struct((tp_n, units, width)),
        ],
        in_specs=[VMEM] * (2 * nx) + [HBM] * 3,
        scratch=[
            pltpu.VMEM((2, width, units), jnp.bfloat16),
            pltpu.VMEM((2, width, units), jnp.bfloat16),
            pltpu.SemaphoreType.DMA((3, tp_n)),
        ],
        mib=20,
    )
    results = kernel(
        functools.partial(late_kernel, nx, tp_n),
        (*[parts[q, m] for q in range(2, tp_n) for m in order], gate, up, *late),
        [struct((slots // nx, width))] * (tp_n * nx),
        mib=20,
    )

    returned = {}
    for g, m in enumerate(order):
        pieces = []
        for q in list(range(2, tp_n, 2)) + [0]:
            own = results[q * nx + g]
            other = shift(results[(q + 1) * nx + g], "tp", 1)
            if q:
                piece = own.astype(jnp.float32) + other.astype(jnp.float32)
                pieces.append(shift(piece.astype(jnp.bfloat16), "tp", q))
            else:
                pieces += [own, other]
        if wide and m == 0:
            returned[0, 0], *mixed = kernel(
                functools.partial(blend_kernel, nz, cap, len(pieces)),
                (*pieces, *outs[1:]),
                [struct((cap, width))]
                + [struct((rows_a + cap * width // wide, wide))] * (nz - 1),
            )
            for k in range(1, nz):
                returned[k, 0] = shift(mixed[k - 1], "ep", k * nx)
        else:
            total = sum(piece.astype(jnp.float32) for piece in pieces).astype(jnp.bfloat16)
            for k in range(nz):
                block = total[k * cap : (k + 1) * cap]
                returned[k, m] = shift(block, "ep", k * nx + m)

    high, low = kernel(
        functools.partial(gates_kernel, nz, nx, cap),
        (routes.T, route_scores.T),
        [struct((slots, rows_b))] * 2,
    )
    shapes = [struct((rows_b, width))] + [struct((rows_a, nz * wide))] * (wide > 0)
    out, *held = kernel(
        functools.partial(finish_kernel, nz, nx, cap, wide),
        (
            high,
            low,
            *[returned[k, m] for k in range(nz) for m in range(nx)],
            *(outs[:1] if wide else ()),
        ),
        shapes,
        out_specs=[HBM] * len(shapes),
        scratch=[
            pltpu.VMEM((slots, width), jnp.bfloat16),
            pltpu.VMEM((rows_b, width), jnp.bfloat16),
            pltpu.SemaphoreType.DMA((nz + 1,)),
        ],
    )
    return held[0] if wide else attended, out


def solution(mesh):
    ep_n, tp_n = mesh.shape["ep"], mesh.shape["tp"]
    nx = 1
    while (2 * nx) * (2 * nx) <= ep_n:
        nx *= 2
    sizes = (ep_n // nx, nx, tp_n)

    def body(*arrays):
        return local(sizes, *arrays)

    return jax.shard_map(
        body,
        mesh=mesh,
        in_specs=(
            P("ep", "tp"),
            P("ep", "tp"),
            P("ep", "tp"),
            P("tp"),
            P(),
            P("ep", None),
            P(),
            P("ep", None),
            P("ep", None),
            P("ep", None, "tp"),
            P("ep", None, "tp"),
            P("ep", "tp", None),
        ),
        out_specs=(P("ep", "tp"), P("ep", "tp")),
        check_vma=False,
    )
```

```python
import functools

import jax
import jax.numpy as jnp
from jax import lax
from jax.experimental import pallas as pl
from jax.experimental.pallas import tpu as pltpu
from jax.sharding import PartitionSpec as P


QKD = 128
VD = 256
TOP = 2


neg_big = -1e30
head_eps = 1e-05
moe_eps = 1e-06
head_scale = 0.8

VMEM = pl.BlockSpec(memory_space=pltpu.VMEM)
SMEM = pl.BlockSpec(memory_space=pltpu.SMEM)
HBM = pl.BlockSpec(memory_space=pltpu.HBM)


def struct(shape, dtype=jnp.bfloat16):
    return jax.ShapeDtypeStruct(shape, dtype)


def params(mib=8):
    return pltpu.CompilerParams(vmem_limit_bytes=mib * 1024 * 1024)


def dot(a, b, contract=((1,), (0,))):
    return lax.dot_general(a, b, (contract, ((), ())), preferred_element_type=jnp.float32)


def where_am_i(nx):
    ep = lax.axis_index("ep")
    return lax.div(ep, nx), lax.rem(ep, nx), lax.axis_index("tp")


def slot_hits(nz, nx, cap, routes):
    z, x, _ = where_am_i(nx)
    blocks, rows = nz * nx, routes.shape[1]
    block = lax.broadcasted_iota(jnp.int32, (blocks, rows), 0)
    wanted = (lax.div(block, nx) ^ z) * nx + (lax.rem(block, nx) ^ x)
    first, second = routes[0:1, :] == wanted, routes[1:2, :] == wanted
    hit = jnp.where(first | second, 1.0, 0.0)
    row_from = lax.broadcasted_iota(jnp.int32, (rows, rows), 0)
    row_to = lax.broadcasted_iota(jnp.int32, (rows, rows), 1)
    before = jnp.where(row_from < row_to, 1.0, 0.0).astype(jnp.bfloat16)
    place = jnp.where(hit > 0.5, dot(hit.astype(jnp.bfloat16), before), -1.0)
    slot = lax.broadcasted_iota(jnp.int32, (blocks, cap, rows), 1).astype(jnp.float32)
    return place[:, None, :] == slot, first


def prep_kernel(nz, nx, cap, width, wide, tokens_ref, gain_ref, routes_ref, *refs):
    blocks = nz * nx
    tokens_s, gain_s, routes_s, sems = refs[-4:]
    copies = [
        pltpu.make_async_copy(routes_ref, routes_s, sems.at[0]),
        pltpu.make_async_copy(tokens_ref, tokens_s, sems.at[1]),
        pltpu.make_async_copy(gain_ref, gain_s, sems.at[2]),
    ]
    slices = []
    if wide:
        z = where_am_i(nx)[0]
        sources, refs = refs[:3], refs[3:]
        count = sources[0].shape[0]
        for k in range(nz):
            columns = pl.ds(pl.multiple_of((z ^ k) * wide, wide), wide)
            for i, source in enumerate(sources):
                target = refs[blocks + k].at[pl.ds(i * count, count), :]
                sem = sems.at[3 + 3 * k + i]
                slices.append(pltpu.make_async_copy(source.at[:, columns], target, sem))
    out_refs = refs[:blocks]
    for copy in copies + slices:
        copy.start()
    rows = tokens_ref.shape[0]
    copies[0].wait()
    picker, _ = slot_hits(nz, nx, cap, routes_s[...])
    picker = jnp.where(picker, 1.0, 0.0).reshape(blocks * cap, rows).astype(jnp.bfloat16)
    for copy in copies[1:]:
        copy.wait()
    tokens = tokens_s[...].astype(jnp.float32)
    scale = lax.rsqrt(jnp.mean(tokens * tokens, axis=-1, keepdims=True) + moe_eps)
    columns = pl.ds(pl.multiple_of(lax.axis_index("tp") * width, width), width)
    normed = tokens_s[:, columns].astype(jnp.float32) * scale * gain_s[:, columns]
    picked = dot(picker, normed.astype(jnp.bfloat16)).astype(jnp.bfloat16)
    for j in range(blocks):
        out_refs[j][...] = picked[j * cap : (j + 1) * cap]
    for copy in slices:
        copy.wait()


def gates_kernel(nz, nx, cap, routes_ref, scores_ref, high_ref, low_ref):
    rows = routes_ref.shape[1]
    scores = scores_ref[...]
    scores = jnp.exp(scores - jnp.max(scores, axis=0, keepdims=True))
    gates = scores / jnp.sum(scores, axis=0, keepdims=True)
    taken, first = slot_hits(nz, nx, cap, routes_ref[...])
    weight = jnp.where(first, gates[0:1, :], gates[1:2, :])
    weight = jnp.where(taken, weight[:, None, :], 0.0).reshape(nz * nx * cap, rows)
    high = weight.astype(jnp.bfloat16)
    high_ref[...] = high
    low_ref[...] = (weight - high.astype(jnp.float32)).astype(jnp.bfloat16)


def total_of(refs):
    total = refs[0][...].astype(jnp.float32)
    for ref in refs[1:]:
        total = total + ref[...].astype(jnp.float32)
    return total.astype(jnp.bfloat16)


def add_kernel(n_sums, *refs):
    total = total_of(refs[:n_sums])
    count = refs[n_sums].shape[0]
    for k, out_ref in enumerate(refs[n_sums:]):
        out_ref[...] = total[k * count : (k + 1) * count]


def blend_kernel(nz, cap, n_sums, *refs):
    sum_refs, refs = refs[:n_sums], refs[n_sums:]
    attend_refs, near_ref, out_refs = refs[: nz - 1], refs[nz - 1], refs[nz:]
    total = total_of(sum_refs)
    near_ref[...] = total[:cap]
    for k in range(1, nz):
        out_ref = out_refs[k - 1]
        count, wide = attend_refs[k - 1].shape
        out_ref[:count, :] = attend_refs[k - 1][...]
        for c in range(total.shape[1] // wide):
            out_ref[count + c * cap : count + (c + 1) * cap, :] = total[
                k * cap : (k + 1) * cap, c * wide : (c + 1) * wide
            ]


def finish_kernel(nz, nx, cap, wide, high_ref, low_ref, *refs):
    blocks, refs = refs[: nz * nx], refs[nz * nx :]
    *refs, held, out_s, sems = refs
    copies = []
    if wide:
        own_ref, out_ref, attended_ref = refs
        z = where_am_i(nx)[0]
        count = own_ref.shape[0]
        for k in range(nz):
            source = blocks[k * nx].at[pl.ds(0, count), :] if k else own_ref
            columns = pl.ds(pl.multiple_of((z ^ k) * wide, wide), wide)
            copies.append(pltpu.make_async_copy(source, attended_ref.at[:, columns], sems.at[k]))
    else:
        (out_ref,) = refs
    for copy in copies:
        copy.start()
    for j, ref in enumerate(blocks):
        slots = slice(j * cap, (j + 1) * cap)
        if wide and j >= nx and j % nx == 0:
            for c in range(held.shape[1] // wide):
                first = count + c * cap
                held[slots, c * wide : (c + 1) * wide] = ref[first : first + cap, :]
        else:
            held[slots, :] = ref[...]
    returned = held[...]
    rows = ((0,), (0,))
    out_s[...] = (
        dot(high_ref[...], returned, rows) + dot(low_ref[...], returned, rows)
    ).astype(jnp.bfloat16)
    copies.append(pltpu.make_async_copy(out_s, out_ref, sems.at[nz]))
    copies[-1].start()
    for copy in copies:
        copy.wait()


def fence_kernel(in_ref, out_ref):
    out_ref[...] = in_ref[...]


def columns_of(q, width):
    return pl.ds(pl.multiple_of((lax.axis_index("tp") ^ q) * width, width), width)


def early_kernel(groups, *refs):
    row_refs, (gate_ref, up_ref), out_refs = (
        refs[: 2 * groups],
        refs[2 * groups : 2 * groups + 2],
        refs[2 * groups + 2 :],
    )
    rows = [
        jnp.concatenate([ref[...] for ref in row_refs[q * groups : (q + 1) * groups]], axis=0)
        for q in range(2)
    ]
    size = row_refs[0].shape[0]
    width = rows[0].shape[1]
    for i, ref in enumerate((gate_ref, up_ref)):
        product = dot(rows[0], ref[columns_of(0, width), :])
        product = product + dot(rows[1], ref[columns_of(1, width), :])
        for g in range(groups):
            out_refs[i * groups + g][...] = product[g * size : (g + 1) * size]


def late_kernel(tp_n, *refs):
    row_refs = refs[: tp_n - 2]
    gate_in, up_in, gate_ref, up_ref, down_ref = refs[tp_n - 2 : tp_n + 3]
    out_refs = refs[tp_n + 3 :]
    gate, up = gate_in[...], up_in[...]
    for q in range(2, tp_n):
        rows = row_refs[q - 2][...]
        gate = gate + dot(rows, gate_ref[columns_of(q, rows.shape[1]), :])
        up = up + dot(rows, up_ref[columns_of(q, rows.shape[1]), :])
    hidden = (gate * jax.nn.sigmoid(gate) * up).astype(jnp.bfloat16)
    for q in range(tp_n):
        block = down_ref[:, columns_of(q, out_refs[q].shape[1])]
        out_refs[q][...] = dot(hidden, block).astype(jnp.bfloat16)


def attend_kernel(nz, nx, heads, lambda_ref, gain_ref, *refs):
    pack_refs, refs = refs[:nz], refs[nz:]
    near_refs, rest_refs, refs = refs[: nx - 1], refs[nx - 1 : 2 * nx - 2], refs[2 * nx - 2 :]
    out_refs = refs[:nz]
    query_s, key_s, value_s, out_s = refs[nz:]
    z, x, _ = where_am_i(nx)
    rows = pack_refs[0].shape[0] // 3

    def at(block):
        return pl.ds(pl.multiple_of(block * rows, rows), rows)

    for k in range(nz):
        query_s[at(z ^ k), :] = pack_refs[k][2 * rows :, :]
        for m in range(nx):
            if m == 0:
                source, first = pack_refs[k], 0
            elif k == 0:
                source, first = near_refs[m - 1], 0
            else:
                source, first = rest_refs[m - 1], (k - 1) * 2 * rows
            block = at((z ^ k) * nx + (x ^ m))
            key_s[block, :] = source[first : first + rows, :]
            value_s[block, :] = source[first + rows : first + 2 * rows, :]
    for head in range(heads):
        weight = lambda_ref[z * heads + head]
        for group in range(nz):
            count = (group + 1) * nx * rows
            query_pos = (group * nx + x) * rows + lax.broadcasted_iota(jnp.int32, (rows, count), 0)
            visible = lax.broadcasted_iota(jnp.int32, (rows, count), 1) <= query_pos
            maps = []
            for index in range(2):
                lanes = slice(head * VD + index * QKD, head * VD + (index + 1) * QKD)
                scores = dot(
                    query_s[group * rows : (group + 1) * rows, lanes],
                    key_s[:count, lanes],
                    ((1,), (1,)),
                )
                scores = jnp.where(visible, scores * QKD ** (-0.5), neg_big)
                weights = jnp.exp(scores - jnp.max(scores, axis=-1, keepdims=True))
                maps.append((weights, jnp.sum(weights, axis=-1, keepdims=True)))
            mixing = maps[0][0] * (1.0 / maps[0][1]) - maps[1][0] * (weight / maps[1][1])
            lanes = slice(head * VD, (head + 1) * VD)
            high = mixing.astype(jnp.bfloat16)
            low = (mixing - high.astype(jnp.float32)).astype(jnp.bfloat16)
            held = value_s[:count, lanes]
            mixed = dot(high, held) + dot(low, held)
            scaled = mixed * lax.rsqrt(jnp.mean(mixed * mixed, axis=-1, keepdims=True) + head_eps)
            scaled = scaled * gain_ref[...] * head_scale
            out_s[group * rows : (group + 1) * rows, lanes] = scaled.astype(jnp.bfloat16)
    for k in range(nz):
        out_refs[k][...] = out_s[at(z ^ k), :]


def fold_block(query_group, query_pos, key_heads, value_heads, key_pos):
    scores = jnp.einsum(
        "qhmd,khmd->hmqk", query_group, key_heads, preferred_element_type=jnp.float32
    ) * QKD ** (-0.5)
    visible = key_pos[None, :] <= query_pos[:, None]
    scores = jnp.where(visible, scores, neg_big)
    weights = jnp.where(visible, jnp.exp(scores - jnp.max(scores, axis=-1, keepdims=True)), 0.0)
    accumulated = jnp.einsum(
        "hmqk,khd->hmqd", weights, value_heads, precision=lax.Precision.HIGHEST
    )
    return jnp.sum(weights, axis=-1), accumulated


def gathered_attention(queries, key_rows, values, lambdas, head_gain):
    rows = queries.shape[0]
    heads = lambdas.shape[0]
    half = rows // 2
    keys = lax.all_gather(key_rows, "ep", axis=0, tiled=True)
    held = lax.all_gather(values, "ep", axis=0, tiled=True)
    count = keys.shape[0]
    keys = keys.reshape(count, heads, 2, QKD)
    held = held.reshape(count, heads, VD).astype(jnp.float32)
    key_pos = jnp.arange(count, dtype=jnp.int32)
    groups = []
    for g in range(2):
        pos = lax.axis_index("ep") * rows + g * half + jnp.arange(half, dtype=jnp.int32)
        group = queries[g * half : (g + 1) * half].reshape(half, heads, 2, QKD)
        total, mixed = fold_block(group, pos, keys, held, key_pos)
        mixed = mixed / total[..., None]
        mixed = mixed[:, 0] - lambdas[:, None, None] * mixed[:, 1]
        scaled = mixed * lax.rsqrt(jnp.mean(mixed * mixed, axis=-1, keepdims=True) + head_eps)
        scaled = scaled * head_gain * head_scale
        groups.append(scaled.transpose(1, 0, 2).reshape(half, heads * VD).astype(jnp.bfloat16))
    return jnp.concatenate(groups, axis=0)


def local(
    sizes,
    queries,
    key_rows,
    values,
    lambdas,
    head_gain,
    tokens,
    moe_gain,
    routes,
    route_scores,
    w_gate,
    w_up,
    w_down,
):
    nz, nx, tp_n = sizes
    ep_n = nz * nx
    rows_b, model = tokens.shape
    cap = 2 * TOP * rows_b // ep_n
    width = model // tp_n
    units = w_gate.shape[2]

    def shift(v, axis, mask):
        if mask == 0:
            return v
        n = ep_n if axis == "ep" else tp_n
        return lax.ppermute(v, axis, [(i, i ^ mask) for i in range(n)])

    def kernel(body, ins, outs, in_specs=None, out_specs=None, scratch=(), mib=8, cost=None):
        if in_specs:
            ins = [
                pltpu.with_memory_space_constraint(v, pltpu.HBM) if spec is HBM else v
                for v, spec in zip(ins, in_specs)
            ]
        return pl.pallas_call(
            body,
            out_shape=outs,
            in_specs=in_specs or [VMEM] * len(ins),
            out_specs=out_specs or jax.tree.map(lambda _: VMEM, outs),
            scratch_shapes=scratch,
            compiler_params=params(mib),
            cost_estimate=cost,
        )(*ins)

    heads, odd = divmod(lambdas.shape[0], nz)
    wide = 0 if odd or width % (heads * VD) else heads * VD
    rows_a = queries.shape[0]
    slices = (key_rows, values, queries) if wide else ()
    sends = kernel(
        functools.partial(prep_kernel, nz, nx, cap, width, wide),
        (tokens, moe_gain.reshape(1, model), routes.T, *slices),
        [struct((cap, width))] * ep_n
        + [struct((3 * rows_a, wide))] * (nz if wide else 0),
        in_specs=[HBM] * (3 + len(slices)),
        scratch=[
            pltpu.VMEM((rows_b, model), jnp.bfloat16),
            pltpu.VMEM((1, model), jnp.float32),
            pltpu.VMEM((TOP, rows_b), jnp.int32),
            pltpu.SemaphoreType.DMA((3 + 3 * nz,)),
        ],
    )
    sends, packs = sends[:ep_n], sends[ep_n:]
    order = list(range(1, nx)) + [0]
    parts = {}
    for m in order:
        arrived = [shift(sends[k * nx + m], "ep", k * nx + m) for k in range(nz)]
        parts[0, m] = jnp.concatenate(arrived, axis=0)

    packs = [shift(pack, "ep", k * nx) for k, pack in enumerate(packs)]

    for q in range(0, tp_n, 2):
        for m in order:
            parts[q, m] = shift(parts[0, m], "tp", q)
            parts[q + 1, m] = shift(parts[q, m], "tp", 1)

    attended = None
    if wide:
        near = packs[0][: 2 * rows_a]
        rest = jnp.concatenate([pack[: 2 * rows_a] for pack in packs[1:]], axis=0)
        near = [shift(near, "ep", m) for m in range(1, nx)]
        rest = [shift(rest, "ep", m) for m in range(1, nx)]
        gain = kernel(fence_kernel, (head_gain.reshape(1, VD),), struct((1, VD), jnp.float32))
        outs = kernel(
            functools.partial(attend_kernel, nz, nx, heads),
            (lambdas, gain, *packs, *near, *rest),
            [struct((rows_a, wide))] * nz,
            in_specs=[SMEM] + [VMEM] * (1 + nz + 2 * (nx - 1)),
            scratch=[
                pltpu.VMEM((nz * rows_a, wide), jnp.bfloat16),
                pltpu.VMEM((ep_n * rows_a, wide), jnp.bfloat16),
                pltpu.VMEM((ep_n * rows_a, wide), jnp.bfloat16),
                pltpu.VMEM((nz * rows_a, wide), jnp.bfloat16),
            ],
            mib=16,
        )
    else:
        attended = gathered_attention(queries, key_rows, values, lambdas, head_gain)

    slots, span = ep_n * cap, nz * cap
    gate, up, down = w_gate[0], w_up[0], w_down[0]
    sums = kernel(
        functools.partial(early_kernel, nx),
        (*[parts[q, m] for q in range(2) for m in order], gate, up),
        [struct((span, units), jnp.float32)] * (2 * nx),
        mib=20,
    )
    results = {}
    for g, m in enumerate(order):
        results[m] = kernel(
            functools.partial(late_kernel, tp_n),
            (*[parts[q, m] for q in range(2, tp_n)], sums[g], sums[nx + g], gate, up, down),
            [struct((span, width))] * tp_n,
            mib=20,
        )

    returned = {}
    for m in order:
        pieces = []
        for q in list(range(2, tp_n, 2)) + [0]:
            both = [results[m][q], shift(results[m][q + 1], "tp", 1)]
            if q:
                (piece,) = kernel(functools.partial(add_kernel, 2), both, [struct((span, width))])
                pieces.append(shift(piece, "tp", q))
            else:
                pieces += both
        if wide and m == 0:
            blocks = kernel(
                functools.partial(blend_kernel, nz, cap, len(pieces)),
                (*pieces, *outs[1:]),
                [struct((cap, width))]
                + [struct((rows_a + cap * width // wide, wide))] * (nz - 1),
            )
        else:
            blocks = kernel(
                functools.partial(add_kernel, len(pieces)), pieces, [struct((cap, width))] * nz
            )
        for k in range(nz):
            returned[k, m] = shift(blocks[k], "ep", k * nx + m)

    high, low = kernel(
        functools.partial(gates_kernel, nz, nx, cap),
        (routes.T, route_scores.T),
        [struct((slots, rows_b))] * 2,
        cost=pl.CostEstimate(flops=20_000_000_000, bytes_accessed=100_000, transcendentals=0),
    )
    shapes = [struct((rows_b, width))] + [struct((rows_a, nz * wide))] * (wide > 0)
    out, *held = kernel(
        functools.partial(finish_kernel, nz, nx, cap, wide),
        (
            high,
            low,
            *[returned[k, m] for k in range(nz) for m in range(nx)],
            *(outs[:1] if wide else ()),
        ),
        shapes,
        out_specs=[HBM] * len(shapes),
        scratch=[
            pltpu.VMEM((slots, width), jnp.bfloat16),
            pltpu.VMEM((rows_b, width), jnp.bfloat16),
            pltpu.SemaphoreType.DMA((nz + 1,)),
        ],
    )
    return held[0] if wide else attended, out


def solution(mesh):
    ep_n, tp_n = mesh.shape["ep"], mesh.shape["tp"]
    nx = 1
    while (2 * nx) * (2 * nx) <= ep_n:
        nx *= 2
    sizes = (ep_n // nx, nx, tp_n)

    def body(*arrays):
        return local(sizes, *arrays)

    return jax.shard_map(
        body,
        mesh=mesh,
        in_specs=(
            P("ep", "tp"),
            P("ep", "tp"),
            P("ep", "tp"),
            P("tp"),
            P(),
            P("ep", None),
            P(),
            P("ep", None),
            P("ep", None),
            P("ep", None, "tp"),
            P("ep", None, "tp"),
            P("ep", "tp", None),
        ),
        out_specs=(P("ep", "tp"), P("ep", "tp")),
        check_vma=False,
    )
```

```python
import functools
import math

import jax
import jax.numpy as jnp
from jax import lax
from jax.experimental import pallas as pl
from jax.experimental.pallas import tpu as pltpu
from jax.sharding import PartitionSpec as P


QKD = 128
VD = 256
TOP = 2


neg_big = -1e30
head_eps = 1e-05
moe_eps = 1e-06
head_scale = 0.8
per_score = QKD ** (-0.5) * math.log2(math.e)

VMEM = pl.BlockSpec(memory_space=pltpu.VMEM)
SMEM = pl.BlockSpec(memory_space=pltpu.SMEM)
HBM = pl.BlockSpec(memory_space=pltpu.HBM)


def struct(shape, dtype=jnp.bfloat16):
    return jax.ShapeDtypeStruct(shape, dtype)


def params(mib=8):
    return pltpu.CompilerParams(vmem_limit_bytes=mib * 1024 * 1024)


def dot(a, b, contract=((1,), (0,))):
    return lax.dot_general(a, b, (contract, ((), ())), preferred_element_type=jnp.float32)


def where_am_i(nx):
    ep = lax.axis_index("ep")
    return lax.div(ep, nx), lax.rem(ep, nx), lax.axis_index("tp")


def columns_of(q, width):
    return pl.ds(pl.multiple_of((lax.axis_index("tp") ^ q) * width, width), width)


def slot_hits(nz, nx, cap, routes):
    z, x, _ = where_am_i(nx)
    blocks, rows = nz * nx, routes.shape[1]
    block = lax.broadcasted_iota(jnp.int32, (blocks, rows), 0)
    wanted = (lax.div(block, nx) ^ z) * nx + (lax.rem(block, nx) ^ x)
    first, second = routes[0:1, :] == wanted, routes[1:2, :] == wanted
    hit = jnp.where(first | second, 1.0, 0.0)
    row_from = lax.broadcasted_iota(jnp.int32, (rows, rows), 0)
    row_to = lax.broadcasted_iota(jnp.int32, (rows, rows), 1)
    before = jnp.where(row_from < row_to, 1.0, 0.0).astype(jnp.bfloat16)
    place = jnp.where(hit > 0.5, dot(hit.astype(jnp.bfloat16), before), -1.0)
    slot = lax.broadcasted_iota(jnp.int32, (blocks, cap, rows), 1).astype(jnp.float32)
    return place[:, None, :] == slot, first


def prep_kernel(nz, nx, cap, width, near, wide, tokens_ref, gain_ref, routes_ref, scores_ref, *refs):
    blocks = nz * nx
    routes_s, scores_s, tokens_s, gain_s, sems = refs[-5:]
    copies = [
        pltpu.make_async_copy(routes_ref, routes_s, sems.at[0]),
        pltpu.make_async_copy(tokens_ref, tokens_s, sems.at[1]),
        pltpu.make_async_copy(gain_ref, gain_s, sems.at[2]),
        pltpu.make_async_copy(scores_ref, scores_s, sems.at[3]),
    ]
    slices = []
    if wide:
        z = where_am_i(nx)[0]
        sources, refs = refs[:3], refs[3:]
        count = sources[0].shape[0]
        for k in range(nz):
            columns = pl.ds(pl.multiple_of((z ^ k) * wide, wide), wide)
            for i, source in enumerate(sources):
                target = refs[blocks + k].at[pl.ds(i * count, count), :]
                sem = sems.at[4 + 3 * k + i]
                slices.append(pltpu.make_async_copy(source.at[:, columns], target, sem))
    out_refs = refs[:blocks]
    for copy in copies + slices:
        copy.start()
    rows = tokens_ref.shape[0]
    copies[0].wait()
    picker, _ = slot_hits(nz, nx, cap, routes_s[...])
    picker = jnp.where(picker, 1.0, 0.0).reshape(blocks * cap, rows).astype(jnp.bfloat16)
    for copy in copies[1:]:
        copy.wait()
    tokens = tokens_s[...].astype(jnp.float32)
    scale = lax.rsqrt(jnp.mean(tokens * tokens, axis=-1, keepdims=True) + moe_eps)
    for q in range(0, tokens.shape[1] // width, 2):
        columns = columns_of(q, width)
        normed = tokens_s[:, columns].astype(jnp.float32) * scale * gain_s[:, columns]
        count = near * nx if q else blocks
        picked = dot(picker[: count * cap], normed.astype(jnp.bfloat16)).astype(jnp.bfloat16)
        for j in range(count):
            out_refs[j][q // 2 * cap : (q // 2 + 1) * cap, :] = picked[j * cap : (j + 1) * cap]
    for copy in slices:
        copy.wait()


def gates_kernel(nz, nx, cap, routes_ref, scores_ref, high_ref, low_ref):
    rows = routes_ref.shape[1]
    scores = scores_ref[...]
    scores = jnp.exp(scores - jnp.max(scores, axis=0, keepdims=True))
    gates = scores / jnp.sum(scores, axis=0, keepdims=True)
    taken, first = slot_hits(nz, nx, cap, routes_ref[...])
    weight = jnp.where(first, gates[0:1, :], gates[1:2, :])
    weight = jnp.where(taken, weight[:, None, :], 0.0).reshape(nz * nx * cap, rows)
    high = weight.astype(jnp.bfloat16)
    high_ref[...] = high
    low_ref[...] = (weight - high.astype(jnp.float32)).astype(jnp.bfloat16)


def total_of(refs, first=0, count=None):
    count = count or refs[0].shape[0]
    total = 0.0
    for ref in refs:
        base = 0 if ref.shape[0] == count else first
        total = total + ref[base : base + count, :].astype(jnp.float32)
    return total.astype(jnp.bfloat16)


def add_kernel(n_sums, first, *refs):
    outs = refs[n_sums:]
    total = total_of(refs[:n_sums], first, sum(ref.shape[0] for ref in outs))
    row = 0
    for out_ref in outs:
        out_ref[...] = total[row : row + out_ref.shape[0]]
        row += out_ref.shape[0]


def finish_kernel(nz, nx, cap, wide, high_ref, low_ref, *refs):
    blocks, refs = refs[: nz * nx], refs[nz * nx :]
    *refs, held, out_s, sems = refs
    copies = []
    if wide:
        *heads, out_ref, attended_ref = refs
        z = where_am_i(nx)[0]
        for k in range(nz):
            columns = pl.ds(pl.multiple_of((z ^ k) * wide, wide), wide)
            copies.append(pltpu.make_async_copy(heads[k], attended_ref.at[:, columns], sems.at[k]))
    else:
        (out_ref,) = refs
    for copy in copies:
        copy.start()
    for j, ref in enumerate(blocks):
        held[j * cap : (j + 1) * cap, :] = ref[...]
    returned = held[...]
    rows = ((0,), (0,))
    out_s[...] = (
        dot(high_ref[...], returned, rows) + dot(low_ref[...], returned, rows)
    ).astype(jnp.bfloat16)
    copies.append(pltpu.make_async_copy(out_s, out_ref, sems.at[nz]))
    copies[-1].start()
    for copy in copies:
        copy.wait()


def fence_kernel(in_ref, out_ref):
    out_ref[...] = in_ref[...]


def early_kernel(first_ref, second_ref, gate_ref, up_ref, *out_refs):
    width = first_ref.shape[1]
    groups = len(out_refs) // 2
    size = first_ref.shape[0] // groups
    for i, ref in enumerate((gate_ref, up_ref)):
        product = dot(first_ref[...], ref[columns_of(0, width), :])
        product = product + dot(second_ref[...], ref[columns_of(1, width), :])
        for g in range(groups):
            out_refs[i * groups + g][...] = product[g * size : (g + 1) * size]


def late_kernel(tp_n, *refs):
    row_refs = refs[: tp_n - 2]
    gate_in, up_in, gate_ref, up_ref, down_ref = refs[tp_n - 2 : tp_n + 3]
    out_refs = refs[tp_n + 3 :]
    gate, up = gate_in[...], up_in[...]
    for q in range(2, tp_n):
        rows = row_refs[q - 2][...]
        gate = gate + dot(rows, gate_ref[columns_of(q, rows.shape[1]), :])
        up = up + dot(rows, up_ref[columns_of(q, rows.shape[1]), :])
    hidden = (gate * jax.nn.sigmoid(gate) * up).astype(jnp.bfloat16)
    for q in range(tp_n):
        block = down_ref[:, columns_of(q, out_refs[q].shape[1])]
        out_refs[q][...] = dot(hidden, block).astype(jnp.bfloat16)


def attend_kernel(nz, nx, heads, swaps, lambda_ref, gain_ref, *refs):
    pack_refs, refs = refs[:nz], refs[nz:]
    count = (nx - 1) * len(swaps)
    swap_refs, refs = refs[:count], refs[count:]
    out_refs = refs[:nz]
    query_s, key_s, value_s, out_s = refs[nz:]
    z, x, _ = where_am_i(nx)
    rows = pack_refs[0].shape[0] // 3

    def at(block):
        return pl.ds(pl.multiple_of(block * rows, rows), rows)

    for k in range(nz):
        query_s[at(z ^ k), :] = pack_refs[k][2 * rows :, :]
        for m in range(nx):
            if m == 0:
                source, first = pack_refs[k], 0
            else:
                i = next(i for i, group in enumerate(swaps) if k in group)
                source, first = swap_refs[i * (nx - 1) + m - 1], swaps[i].index(k) * 2 * rows
            block = at((z ^ k) * nx + (x ^ m))
            key_s[block, :] = source[first : first + rows, :]
            value_s[block, :] = source[first + rows : first + 2 * rows, :]
    for head in range(heads):
        weight = lambda_ref[z * heads + head]
        for group in range(nz):
            count, last = (group + 1) * nx * rows, nx * rows
            query_pos = x * rows + lax.broadcasted_iota(jnp.int32, (rows, last), 0)
            visible = lax.broadcasted_iota(jnp.int32, (rows, last), 1) <= query_pos
            maps = []
            for index in range(2):
                lanes = slice(head * VD + index * QKD, head * VD + (index + 1) * QKD)
                scores = dot(
                    query_s[group * rows : (group + 1) * rows, lanes],
                    key_s[:count, lanes],
                    ((1,), (1,)),
                )
                diagonal = jnp.where(visible, scores[:, count - last :], neg_big)
                if group:
                    diagonal = jnp.concatenate([scores[:, : count - last], diagonal], axis=1)
                scores = diagonal
                weights = jnp.exp2((scores - jnp.max(scores, axis=-1, keepdims=True)) * per_score)
                maps.append((weights, jnp.sum(weights, axis=-1, keepdims=True)))
            mixing = maps[0][0] * (1.0 / maps[0][1]) - maps[1][0] * (weight / maps[1][1])
            lanes = slice(head * VD, (head + 1) * VD)
            mixed = dot(mixing.astype(jnp.bfloat16), value_s[:count, lanes])
            scaled = mixed * lax.rsqrt(jnp.mean(mixed * mixed, axis=-1, keepdims=True) + head_eps)
            scaled = scaled * gain_ref[...] * head_scale
            out_s[group * rows : (group + 1) * rows, lanes] = scaled.astype(jnp.bfloat16)
    for k in range(nz):
        out_refs[k][...] = out_s[at(z ^ k), :]


def fold_block(query_group, query_pos, key_heads, value_heads, key_pos):
    scores = jnp.einsum(
        "qhmd,khmd->hmqk", query_group, key_heads, preferred_element_type=jnp.float32
    ) * QKD ** (-0.5)
    visible = key_pos[None, :] <= query_pos[:, None]
    scores = jnp.where(visible, scores, neg_big)
    weights = jnp.where(visible, jnp.exp(scores - jnp.max(scores, axis=-1, keepdims=True)), 0.0)
    accumulated = jnp.einsum(
        "hmqk,khd->hmqd", weights, value_heads, precision=lax.Precision.HIGHEST
    )
    return jnp.sum(weights, axis=-1), accumulated


def gathered_attention(queries, key_rows, values, lambdas, head_gain):
    rows = queries.shape[0]
    heads = lambdas.shape[0]
    half = rows // 2
    keys = lax.all_gather(key_rows, "ep", axis=0, tiled=True)
    held = lax.all_gather(values, "ep", axis=0, tiled=True)
    count = keys.shape[0]
    keys = keys.reshape(count, heads, 2, QKD)
    held = held.reshape(count, heads, VD).astype(jnp.float32)
    key_pos = jnp.arange(count, dtype=jnp.int32)
    groups = []
    for g in range(2):
        pos = lax.axis_index("ep") * rows + g * half + jnp.arange(half, dtype=jnp.int32)
        group = queries[g * half : (g + 1) * half].reshape(half, heads, 2, QKD)
        total, mixed = fold_block(group, pos, keys, held, key_pos)
        mixed = mixed / total[..., None]
        mixed = mixed[:, 0] - lambdas[:, None, None] * mixed[:, 1]
        scaled = mixed * lax.rsqrt(jnp.mean(mixed * mixed, axis=-1, keepdims=True) + head_eps)
        scaled = scaled * head_gain * head_scale
        groups.append(scaled.transpose(1, 0, 2).reshape(half, heads * VD).astype(jnp.bfloat16))
    return jnp.concatenate(groups, axis=0)


def local(
    sizes,
    queries,
    key_rows,
    values,
    lambdas,
    head_gain,
    tokens,
    moe_gain,
    routes,
    route_scores,
    w_gate,
    w_up,
    w_down,
):
    nz, nx, tp_n = sizes
    ep_n = nz * nx
    rows_b, model = tokens.shape
    cap = 2 * TOP * rows_b // ep_n
    width = model // tp_n
    units = w_gate.shape[2]

    def shift(v, axis, mask):
        if mask == 0:
            return v
        n = ep_n if axis == "ep" else tp_n
        return lax.ppermute(v, axis, [(i, i ^ mask) for i in range(n)])

    def kernel(body, ins, outs, in_specs=None, out_specs=None, scratch=(), mib=8, cost=None):
        if in_specs:
            ins = [
                pltpu.with_memory_space_constraint(v, pltpu.HBM) if spec is HBM else v
                for v, spec in zip(ins, in_specs)
            ]
        return pl.pallas_call(
            body,
            out_shape=outs,
            in_specs=in_specs or [VMEM] * len(ins),
            out_specs=out_specs or jax.tree.map(lambda _: VMEM, outs),
            scratch_shapes=scratch,
            compiler_params=params(mib),
            cost_estimate=cost,
        )(*ins)

    heads, odd = divmod(lambdas.shape[0], nz)
    wide = 0 if odd or width % (heads * VD) else heads * VD
    rows_a = queries.shape[0]
    slices = (key_rows, values, queries) if wide else ()
    near = min(2, nz)
    sends = kernel(
        functools.partial(prep_kernel, nz, nx, cap, width, near, wide),
        (tokens, moe_gain.reshape(1, model), routes.T, route_scores.T, *slices),
        [struct(((tp_n // 2 if j < near * nx else 1) * cap, width)) for j in range(ep_n)]
        + [struct((3 * rows_a, wide))] * (nz if wide else 0)
        + [struct((TOP, rows_b), jnp.int32), struct((TOP, rows_b), jnp.float32)],
        in_specs=[HBM] * (4 + len(slices)),
        scratch=[
            pltpu.VMEM((rows_b, model), jnp.bfloat16),
            pltpu.VMEM((1, model), jnp.float32),
            pltpu.SemaphoreType.DMA((4 + 3 * nz,)),
        ],
    )
    *sends, routes_v, scores_v = sends
    sends, packs = sends[:ep_n], sends[ep_n:]
    order = list(range(1, nx)) + [0]
    parts = {}
    for m in order:
        arrived = [shift(sends[k * nx + m], "ep", k * nx + m) for k in range(nz)]
        far = jnp.concatenate(arrived[near:], axis=0)
        for q in range(0, tp_n, 2):
            pieces = [block[q // 2 * cap : (q // 2 + 1) * cap] for block in arrived[:near]]
            pieces.append(shift(far, "tp", q))
            parts[q, m] = jnp.concatenate(pieces, axis=0)
            if q:
                parts[q + 1, m] = shift(parts[q, m], "tp", 1)
    first = jnp.concatenate([parts[0, m] for m in order], axis=0)
    second = shift(first, "tp", 1)

    packs = [shift(pack, "ep", k * nx) for k, pack in enumerate(packs)]

    attended = None
    if wide:
        swaps = [[0], [nz // 2], [k for k in range(1, nz) if k != nz // 2]]
        swapped = []
        for group in swaps:
            pairs = jnp.concatenate([packs[k][: 2 * rows_a] for k in group], axis=0)
            swapped += [shift(pairs, "ep", m) for m in range(1, nx)]
        gain = kernel(fence_kernel, (head_gain.reshape(1, VD),), struct((1, VD), jnp.float32))
        outs = kernel(
            functools.partial(attend_kernel, nz, nx, heads, swaps),
            (lambdas, gain, *packs, *swapped),
            [struct((rows_a, wide))] * nz,
            in_specs=[SMEM] + [VMEM] * (1 + nz + len(swapped)),
            scratch=[
                pltpu.VMEM((nz * rows_a, wide), jnp.bfloat16),
                pltpu.VMEM((ep_n * rows_a, wide), jnp.bfloat16),
                pltpu.VMEM((ep_n * rows_a, wide), jnp.bfloat16),
                pltpu.VMEM((nz * rows_a, wide), jnp.bfloat16),
            ],
            mib=16,
        )
        outs = [shift(outs[k], "ep", k * nx) for k in range(nz)]
    else:
        attended = gathered_attention(queries, key_rows, values, lambdas, head_gain)

    slots, span = ep_n * cap, nz * cap
    gate, up, down = w_gate[0], w_up[0], w_down[0]
    sums = kernel(
        early_kernel,
        (first, second, gate, up),
        [struct((span, units), jnp.float32)] * (2 * nx),
        mib=20,
    )
    results = {}
    for g, m in enumerate(order):
        results[m] = kernel(
            functools.partial(late_kernel, tp_n),
            (*[parts[q, m] for q in range(2, tp_n)], sums[g], sums[nx + g], gate, up, down),
            [struct((span, width))] * tp_n,
            mib=20,
        )

    returned = {}
    for m in order:
        other = [shift(results[m][q + 1], "tp", 1) for q in range(0, tp_n, 2)]
        bounds = [0, nz] if m == 0 or near == nz else [0, near, nz]
        sizes = [(b - a) * cap for a, b in zip(bounds, bounds[1:])]
        crossed = {i: [] for i in range(len(sizes))}
        for q in range(2, tp_n, 2):
            pieces = kernel(
                functools.partial(add_kernel, 2, 0),
                (results[m][q], other[q // 2]),
                [struct((size, width)) for size in sizes],
            )
            for i, piece in enumerate(pieces):
                crossed[i].append(shift(piece, "tp", q))
        for i, size in enumerate(sizes):
            pieces = (*crossed[i], results[m][0], other[0])
            blocks = kernel(
                functools.partial(add_kernel, len(pieces), bounds[i] * cap),
                pieces,
                [struct((cap, width))] * (size // cap),
            )
            for k, block in enumerate(blocks, bounds[i]):
                returned[k, m] = shift(block, "ep", k * nx + m)

    high, low = kernel(
        functools.partial(gates_kernel, nz, nx, cap),
        (routes_v, scores_v),
        [struct((slots, rows_b))] * 2,
        cost=pl.CostEstimate(flops=20_000_000_000, bytes_accessed=100_000, transcendentals=0),
    )
    shapes = [struct((rows_b, width))] + [struct((rows_a, nz * wide))] * (wide > 0)
    out, *held = kernel(
        functools.partial(finish_kernel, nz, nx, cap, wide),
        (
            high,
            low,
            *[returned[k, m] for k in range(nz) for m in range(nx)],
            *(outs if wide else ()),
        ),
        shapes,
        out_specs=[HBM] * len(shapes),
        scratch=[
            pltpu.VMEM((slots, width), jnp.bfloat16),
            pltpu.VMEM((rows_b, width), jnp.bfloat16),
            pltpu.SemaphoreType.DMA((nz + 1,)),
        ],
    )
    return held[0] if wide else attended, out


def solution(mesh):
    ep_n, tp_n = mesh.shape["ep"], mesh.shape["tp"]
    nx = 1
    while (2 * nx) * (2 * nx) <= ep_n:
        nx *= 2
    sizes = (ep_n // nx, nx, tp_n)

    def body(*arrays):
        return local(sizes, *arrays)

    return jax.shard_map(
        body,
        mesh=mesh,
        in_specs=(
            P("ep", "tp"),
            P("ep", "tp"),
            P("ep", "tp"),
            P("tp"),
            P(),
            P("ep", None),
            P(),
            P("ep", None),
            P("ep", None),
            P("ep", None, "tp"),
            P("ep", None, "tp"),
            P("ep", "tp", None),
        ),
        out_specs=(P("ep", "tp"), P("ep", "tp")),
        check_vma=False,
    )
```

```python
import functools
import math

import jax
import jax.numpy as jnp
from jax import lax
from jax.experimental import pallas as pl
from jax.experimental.pallas import tpu as pltpu
from jax.sharding import PartitionSpec as P


QKD = 128
VD = 256
TOP = 2


neg_big = -1e30
head_eps = 1e-05
moe_eps = 1e-06
head_scale = 0.8
per_score = QKD ** (-0.5) * math.log2(math.e)

VMEM = pl.BlockSpec(memory_space=pltpu.VMEM)
SMEM = pl.BlockSpec(memory_space=pltpu.SMEM)
HBM = pl.BlockSpec(memory_space=pltpu.HBM)


def struct(shape, dtype=jnp.bfloat16):
    return jax.ShapeDtypeStruct(shape, dtype)


def params(mib=8):
    return pltpu.CompilerParams(vmem_limit_bytes=mib * 1024 * 1024)


def dot(a, b, contract=((1,), (0,))):
    return lax.dot_general(a, b, (contract, ((), ())), preferred_element_type=jnp.float32)


def where_am_i(nx):
    ep = lax.axis_index("ep")
    return lax.div(ep, nx), lax.rem(ep, nx), lax.axis_index("tp")


def columns_of(q, width):
    return pl.ds(pl.multiple_of((lax.axis_index("tp") ^ q) * width, width), width)


def slot_hits(nz, nx, cap, routes):
    z, x, _ = where_am_i(nx)
    blocks, rows = nz * nx, routes.shape[1]
    block = lax.broadcasted_iota(jnp.int32, (blocks, rows), 0)
    wanted = (lax.div(block, nx) ^ z) * nx + (lax.rem(block, nx) ^ x)
    first, second = routes[0:1, :] == wanted, routes[1:2, :] == wanted
    hit = jnp.where(first | second, 1.0, 0.0)
    row_from = lax.broadcasted_iota(jnp.int32, (rows, rows), 0)
    row_to = lax.broadcasted_iota(jnp.int32, (rows, rows), 1)
    before = jnp.where(row_from < row_to, 1.0, 0.0).astype(jnp.bfloat16)
    place = jnp.where(hit > 0.5, dot(hit.astype(jnp.bfloat16), before), -1.0)
    slot = lax.broadcasted_iota(jnp.int32, (blocks, cap, rows), 1).astype(jnp.float32)
    return place[:, None, :] == slot, first


def prep_kernel(nz, nx, cap, width, near, wide, tokens_ref, gain_ref, routes_ref, scores_ref, *refs):
    blocks = nz * nx
    routes_s, scores_s, tokens_s, gain_s, sems = refs[-5:]
    copies = [
        pltpu.make_async_copy(routes_ref, routes_s, sems.at[0]),
        pltpu.make_async_copy(tokens_ref, tokens_s, sems.at[1]),
        pltpu.make_async_copy(gain_ref, gain_s, sems.at[2]),
        pltpu.make_async_copy(scores_ref, scores_s, sems.at[3]),
    ]
    slices = []
    if wide:
        z = where_am_i(nx)[0]
        sources, refs = refs[:3], refs[3:]
        count = sources[0].shape[0]
        for k in range(nz):
            columns = pl.ds(pl.multiple_of((z ^ k) * wide, wide), wide)
            for i, source in enumerate(sources):
                target = refs[blocks + k].at[pl.ds(i * count, count), :]
                sem = sems.at[4 + 3 * k + i]
                slices.append(pltpu.make_async_copy(source.at[:, columns], target, sem))
    out_refs = refs[:blocks]
    for copy in copies + slices:
        copy.start()
    rows = tokens_ref.shape[0]
    copies[0].wait()
    picker, _ = slot_hits(nz, nx, cap, routes_s[...])
    picker = jnp.where(picker, 1.0, 0.0).reshape(blocks * cap, rows).astype(jnp.bfloat16)
    for copy in copies[1:]:
        copy.wait()
    tokens = tokens_s[...].astype(jnp.float32)
    scale = lax.rsqrt(jnp.mean(tokens * tokens, axis=-1, keepdims=True) + moe_eps)
    for q in range(0, tokens.shape[1] // width, 2):
        columns = columns_of(q, width)
        normed = tokens_s[:, columns].astype(jnp.float32) * scale * gain_s[:, columns]
        count = near * nx if q else blocks
        picked = dot(picker[: count * cap], normed.astype(jnp.bfloat16)).astype(jnp.bfloat16)
        for j in range(count):
            out_refs[j][q // 2 * cap : (q // 2 + 1) * cap, :] = picked[j * cap : (j + 1) * cap]
    for copy in slices:
        copy.wait()


def gates_kernel(nz, nx, cap, routes_ref, scores_ref, high_ref, low_ref):
    rows = routes_ref.shape[1]
    scores = scores_ref[...]
    scores = jnp.exp(scores - jnp.max(scores, axis=0, keepdims=True))
    gates = scores / jnp.sum(scores, axis=0, keepdims=True)
    taken, first = slot_hits(nz, nx, cap, routes_ref[...])
    weight = jnp.where(first, gates[0:1, :], gates[1:2, :])
    weight = jnp.where(taken, weight[:, None, :], 0.0).reshape(nz * nx * cap, rows)
    high = weight.astype(jnp.bfloat16)
    high_ref[...] = high
    low_ref[...] = (weight - high.astype(jnp.float32)).astype(jnp.bfloat16)


def total_of(refs, first=0, count=None):
    count = count or refs[0].shape[0]
    total = 0.0
    for ref in refs:
        base = 0 if ref.shape[0] == count else first
        total = total + ref[base : base + count, :].astype(jnp.float32)
    return total.astype(jnp.bfloat16)


def add_kernel(n_sums, first, *refs):
    outs = refs[n_sums:]
    total = total_of(refs[:n_sums], first, sum(ref.shape[0] for ref in outs))
    row = 0
    for out_ref in outs:
        out_ref[...] = total[row : row + out_ref.shape[0]]
        row += out_ref.shape[0]


def combine_kernel(cap, high_ref, low_ref, *refs):
    *blocks, out_ref, held, out_s, sem = refs
    for j, ref in enumerate(blocks):
        held[j * cap : (j + 1) * cap, :] = ref[...]
    returned = held[...]
    rows = ((0,), (0,))
    out_s[...] = (
        dot(high_ref[...], returned, rows) + dot(low_ref[...], returned, rows)
    ).astype(jnp.bfloat16)
    copy = pltpu.make_async_copy(out_s, out_ref, sem)
    copy.start()
    copy.wait()


def join_kernel(nz, nx, *refs):
    *head_refs, out_ref, sems = refs
    z = where_am_i(nx)[0]
    wide = head_refs[0].shape[1]
    copies = []
    for k in range(nz):
        columns = pl.ds(pl.multiple_of((z ^ k) * wide, wide), wide)
        copies.append(pltpu.make_async_copy(head_refs[k], out_ref.at[:, columns], sems.at[k]))
    for copy in copies:
        copy.start()
    for copy in copies:
        copy.wait()


def fence_kernel(in_ref, out_ref):
    out_ref[...] = in_ref[...]


def early_kernel(first_ref, second_ref, gate_ref, up_ref, *out_refs):
    width = first_ref.shape[1]
    groups = len(out_refs) // 2
    size = first_ref.shape[0] // groups
    for i, ref in enumerate((gate_ref, up_ref)):
        product = dot(first_ref[...], ref[columns_of(0, width), :])
        product = product + dot(second_ref[...], ref[columns_of(1, width), :])
        for g in range(groups):
            out_refs[i * groups + g][...] = product[g * size : (g + 1) * size]


def late_kernel(tp_n, *refs):
    row_refs = refs[: tp_n - 2]
    gate_in, up_in, gate_ref, up_ref, down_ref = refs[tp_n - 2 : tp_n + 3]
    out_refs = refs[tp_n + 3 :]
    gate, up = gate_in[...], up_in[...]
    for q in range(2, tp_n):
        rows = row_refs[q - 2][...]
        gate = gate + dot(rows, gate_ref[columns_of(q, rows.shape[1]), :])
        up = up + dot(rows, up_ref[columns_of(q, rows.shape[1]), :])
    hidden = (gate * jax.nn.sigmoid(gate) * up).astype(jnp.bfloat16)
    for q in range(tp_n):
        block = down_ref[:, columns_of(q, out_refs[q].shape[1])]
        out_refs[q][...] = dot(hidden, block).astype(jnp.bfloat16)


def attend_kernel(nz, nx, heads, swaps, lambda_ref, gain_ref, *refs):
    pack_refs, refs = refs[:nz], refs[nz:]
    count = (nx - 1) * len(swaps)
    swap_refs, refs = refs[:count], refs[count:]
    out_refs = refs[:nz]
    query_s, key_s, value_s, out_s = refs[nz:]
    z, x, _ = where_am_i(nx)
    rows = pack_refs[0].shape[0] // 3

    def at(block):
        return pl.ds(pl.multiple_of(block * rows, rows), rows)

    for k in range(nz):
        query_s[at(z ^ k), :] = pack_refs[k][2 * rows :, :]
        for m in range(nx):
            if m == 0:
                source, first = pack_refs[k], 0
            else:
                i = next(i for i, group in enumerate(swaps) if k in group)
                source, first = swap_refs[i * (nx - 1) + m - 1], swaps[i].index(k) * 2 * rows
            block = at((z ^ k) * nx + (x ^ m))
            key_s[block, :] = source[first : first + rows, :]
            value_s[block, :] = source[first + rows : first + 2 * rows, :]
    for head in range(heads):
        weight = lambda_ref[z * heads + head]
        for group in range(nz):
            count, last = (group + 1) * nx * rows, nx * rows
            query_pos = x * rows + lax.broadcasted_iota(jnp.int32, (rows, last), 0)
            visible = lax.broadcasted_iota(jnp.int32, (rows, last), 1) <= query_pos
            maps = []
            for index in range(2):
                lanes = slice(head * VD + index * QKD, head * VD + (index + 1) * QKD)
                scores = dot(
                    query_s[group * rows : (group + 1) * rows, lanes],
                    key_s[:count, lanes],
                    ((1,), (1,)),
                )
                diagonal = jnp.where(visible, scores[:, count - last :], neg_big)
                if group:
                    diagonal = jnp.concatenate([scores[:, : count - last], diagonal], axis=1)
                scores = diagonal
                weights = jnp.exp2((scores - jnp.max(scores, axis=-1, keepdims=True)) * per_score)
                maps.append((weights, jnp.sum(weights, axis=-1, keepdims=True)))
            mixing = maps[0][0] * (1.0 / maps[0][1]) - maps[1][0] * (weight / maps[1][1])
            lanes = slice(head * VD, (head + 1) * VD)
            mixed = dot(mixing.astype(jnp.bfloat16), value_s[:count, lanes])
            scaled = mixed * lax.rsqrt(jnp.mean(mixed * mixed, axis=-1, keepdims=True) + head_eps)
            scaled = scaled * gain_ref[...] * head_scale
            out_s[group * rows : (group + 1) * rows, lanes] = scaled.astype(jnp.bfloat16)
    for k in range(nz):
        out_refs[k][...] = out_s[at(z ^ k), :]


def fold_block(query_group, query_pos, key_heads, value_heads, key_pos):
    scores = jnp.einsum(
        "qhmd,khmd->hmqk", query_group, key_heads, preferred_element_type=jnp.float32
    ) * QKD ** (-0.5)
    visible = key_pos[None, :] <= query_pos[:, None]
    scores = jnp.where(visible, scores, neg_big)
    weights = jnp.where(visible, jnp.exp(scores - jnp.max(scores, axis=-1, keepdims=True)), 0.0)
    accumulated = jnp.einsum(
        "hmqk,khd->hmqd", weights, value_heads, precision=lax.Precision.HIGHEST
    )
    return jnp.sum(weights, axis=-1), accumulated


def gathered_attention(queries, key_rows, values, lambdas, head_gain):
    rows = queries.shape[0]
    heads = lambdas.shape[0]
    half = rows // 2
    keys = lax.all_gather(key_rows, "ep", axis=0, tiled=True)
    held = lax.all_gather(values, "ep", axis=0, tiled=True)
    count = keys.shape[0]
    keys = keys.reshape(count, heads, 2, QKD)
    held = held.reshape(count, heads, VD).astype(jnp.float32)
    key_pos = jnp.arange(count, dtype=jnp.int32)
    groups = []
    for g in range(2):
        pos = lax.axis_index("ep") * rows + g * half + jnp.arange(half, dtype=jnp.int32)
        group = queries[g * half : (g + 1) * half].reshape(half, heads, 2, QKD)
        total, mixed = fold_block(group, pos, keys, held, key_pos)
        mixed = mixed / total[..., None]
        mixed = mixed[:, 0] - lambdas[:, None, None] * mixed[:, 1]
        scaled = mixed * lax.rsqrt(jnp.mean(mixed * mixed, axis=-1, keepdims=True) + head_eps)
        scaled = scaled * head_gain * head_scale
        groups.append(scaled.transpose(1, 0, 2).reshape(half, heads * VD).astype(jnp.bfloat16))
    return jnp.concatenate(groups, axis=0)


def local(
    sizes,
    queries,
    key_rows,
    values,
    lambdas,
    head_gain,
    tokens,
    moe_gain,
    routes,
    route_scores,
    w_gate,
    w_up,
    w_down,
):
    nz, nx, tp_n = sizes
    ep_n = nz * nx
    rows_b, model = tokens.shape
    cap = 2 * TOP * rows_b // ep_n
    width = model // tp_n
    units = w_gate.shape[2]

    def shift(v, axis, mask):
        if mask == 0:
            return v
        n = ep_n if axis == "ep" else tp_n
        return lax.ppermute(v, axis, [(i, i ^ mask) for i in range(n)])

    def kernel(body, ins, outs, in_specs=None, out_specs=None, scratch=(), mib=8, cost=None):
        if in_specs:
            ins = [
                pltpu.with_memory_space_constraint(v, pltpu.HBM) if spec is HBM else v
                for v, spec in zip(ins, in_specs)
            ]
        return pl.pallas_call(
            body,
            out_shape=outs,
            in_specs=in_specs or [VMEM] * len(ins),
            out_specs=out_specs or jax.tree.map(lambda _: VMEM, outs),
            scratch_shapes=scratch,
            compiler_params=params(mib),
            cost_estimate=cost,
        )(*ins)

    heads, odd = divmod(lambdas.shape[0], nz)
    wide = 0 if odd or width % (heads * VD) else heads * VD
    rows_a = queries.shape[0]
    slices = (key_rows, values, queries) if wide else ()
    near = min(2, nz)
    sends = kernel(
        functools.partial(prep_kernel, nz, nx, cap, width, near, wide),
        (tokens, moe_gain.reshape(1, model), routes.T, route_scores.T, *slices),
        [struct(((tp_n // 2 if j < near * nx else 1) * cap, width)) for j in range(ep_n)]
        + [struct((3 * rows_a, wide))] * (nz if wide else 0)
        + [struct((TOP, rows_b), jnp.int32), struct((TOP, rows_b), jnp.float32)],
        in_specs=[HBM] * (4 + len(slices)),
        scratch=[
            pltpu.VMEM((rows_b, model), jnp.bfloat16),
            pltpu.VMEM((1, model), jnp.float32),
            pltpu.SemaphoreType.DMA((4 + 3 * nz,)),
        ],
    )
    *sends, routes_v, scores_v = sends
    sends, packs = sends[:ep_n], sends[ep_n:]
    order = list(range(1, nx)) + [0]
    parts = {}
    for m in order:
        arrived = [shift(sends[k * nx + m], "ep", k * nx + m) for k in range(nz)]
        far = jnp.concatenate(arrived[near:], axis=0)
        for q in range(0, tp_n, 2):
            pieces = [block[q // 2 * cap : (q // 2 + 1) * cap] for block in arrived[:near]]
            pieces.append(shift(far, "tp", q))
            parts[q, m] = jnp.concatenate(pieces, axis=0)
            if q:
                parts[q + 1, m] = shift(parts[q, m], "tp", 1)
    first = jnp.concatenate([parts[0, m] for m in order], axis=0)
    second = shift(first, "tp", 1)

    packs = [shift(pack, "ep", k * nx) for k, pack in enumerate(packs)]

    if wide:
        swaps = [[0], [nz // 2], [k for k in range(1, nz) if k != nz // 2]]
        swapped = []
        for group in swaps:
            pairs = jnp.concatenate([packs[k][: 2 * rows_a] for k in group], axis=0)
            swapped += [shift(pairs, "ep", m) for m in range(1, nx)]
        gain = kernel(fence_kernel, (head_gain.reshape(1, VD),), struct((1, VD), jnp.float32))
        outs = kernel(
            functools.partial(attend_kernel, nz, nx, heads, swaps),
            (lambdas, gain, *packs, *swapped),
            [struct((rows_a, wide))] * nz,
            in_specs=[SMEM] + [VMEM] * (1 + nz + len(swapped)),
            scratch=[
                pltpu.VMEM((nz * rows_a, wide), jnp.bfloat16),
                pltpu.VMEM((ep_n * rows_a, wide), jnp.bfloat16),
                pltpu.VMEM((ep_n * rows_a, wide), jnp.bfloat16),
                pltpu.VMEM((nz * rows_a, wide), jnp.bfloat16),
            ],
            mib=16,
        )
        outs = [shift(outs[k], "ep", k * nx) for k in range(nz)]
        attended = kernel(
            functools.partial(join_kernel, nz, nx),
            outs,
            struct((rows_a, nz * wide)),
            out_specs=HBM,
            scratch=[pltpu.SemaphoreType.DMA((nz,))],
        )
    else:
        attended = gathered_attention(queries, key_rows, values, lambdas, head_gain)

    slots, span = ep_n * cap, nz * cap
    gate, up, down = w_gate[0], w_up[0], w_down[0]
    sums = kernel(
        early_kernel,
        (first, second, gate, up),
        [struct((span, units), jnp.float32)] * (2 * nx),
        mib=20,
    )
    results = {}
    for g, m in enumerate(order):
        results[m] = kernel(
            functools.partial(late_kernel, tp_n),
            (*[parts[q, m] for q in range(2, tp_n)], sums[g], sums[nx + g], gate, up, down),
            [struct((span, width))] * tp_n,
            mib=20,
        )

    returned = {}
    for m in order:
        other = [shift(results[m][q + 1], "tp", 1) for q in range(0, tp_n, 2)]
        bounds = [0, nz] if m == 0 or near == nz else [0, near, nz]
        sizes = [(b - a) * cap for a, b in zip(bounds, bounds[1:])]
        crossed = {i: [] for i in range(len(sizes))}
        for q in range(2, tp_n, 2):
            pieces = kernel(
                functools.partial(add_kernel, 2, 0),
                (results[m][q], other[q // 2]),
                [struct((size, width)) for size in sizes],
            )
            for i, piece in enumerate(pieces):
                crossed[i].append(shift(piece, "tp", q))
        for i, size in enumerate(sizes):
            pieces = (*crossed[i], results[m][0], other[0])
            blocks = kernel(
                functools.partial(add_kernel, len(pieces), bounds[i] * cap),
                pieces,
                [struct((cap, width))] * (size // cap),
            )
            for k, block in enumerate(blocks, bounds[i]):
                returned[k, m] = shift(block, "ep", k * nx + m)

    high, low = kernel(
        functools.partial(gates_kernel, nz, nx, cap),
        (routes_v, scores_v),
        [struct((slots, rows_b))] * 2,
        cost=pl.CostEstimate(flops=20_000_000_000, bytes_accessed=100_000, transcendentals=0),
    )
    out = kernel(
        functools.partial(combine_kernel, cap),
        (high, low, *[returned[k, m] for k in range(nz) for m in range(nx)]),
        struct((rows_b, width)),
        out_specs=HBM,
        scratch=[
            pltpu.VMEM((slots, width), jnp.bfloat16),
            pltpu.VMEM((rows_b, width), jnp.bfloat16),
            pltpu.SemaphoreType.DMA,
        ],
    )
    return attended, out


def solution(mesh):
    ep_n, tp_n = mesh.shape["ep"], mesh.shape["tp"]
    nx = 1
    while (2 * nx) * (2 * nx) <= ep_n:
        nx *= 2
    sizes = (ep_n // nx, nx, tp_n)

    def body(*arrays):
        return local(sizes, *arrays)

    return jax.shard_map(
        body,
        mesh=mesh,
        in_specs=(
            P("ep", "tp"),
            P("ep", "tp"),
            P("ep", "tp"),
            P("tp"),
            P(),
            P("ep", None),
            P(),
            P("ep", None),
            P("ep", None),
            P("ep", None, "tp"),
            P("ep", None, "tp"),
            P("ep", "tp", None),
        ),
        out_specs=(P("ep", "tp"), P("ep", "tp")),
        check_vma=False,
    )
```
